128 devices in a mesh: sp: 16 (over z, y), tp: 8 (over x, core).
Axes of the slice: x: 4, y: 4, z: 4, core: 2. Of those that a mesh axis runs over, the one named last changes fastest.
Arguments:
- resid: bfloat16 [16384, 2048], P(('sp', 'tp')), may hold values from -6 to 6
- queries: bfloat16 [16384, 2048], P('sp', 'tp'), may hold values from -6 to 6
- keys: bfloat16 [16384, 2048], P('sp', 'tp'), may hold values from -6 to 6
- values: bfloat16 [16384, 4096], P('sp', 'tp'), may hold values from -6 to 6
- gates: bfloat16 [16384, 4096], P('sp', 'tp'), may hold values from -6 to 6
- log_decay: float32 [8, 16384], P('tp', 'sp'), may hold values from -1 to 0
- retention_output_weight: bfloat16 [4096, 2048], P('tp'), may hold values from -0.125 to 0.125
- norm_gain: bfloat16 [2048], replicated, may hold values from 0.099609375 to 1.8984375
- up_weight: bfloat16 [2048, 8192], P('sp', 'tp'), may hold values from -0.125 to 0.125
- down_weight: bfloat16 [8192, 2048], P('tp', 'sp'), may hold values from -0.0625 to 0.0625
Outputs:
- layer_out: bfloat16 [16384, 2048], P(('sp', 'tp'))
The draws below stay inside these ranges and needn't reach their ends.
All inputs are finite; a program needn't handle non-finite values.
Results may differ from the reference program's by a relative error of at most 0.02.
Values may be sent and summed in bfloat16 or wider, within the bound.
A program may use at most 128 MiB of HBM per device.

```python
import math
import jax
import jax.numpy as jnp
from jax import lax

D = 2048
HEADS = 8
DK = 256
DV = 512
FF = 8192
BLOCK = 128
TOK_DEV = 1024
SEQ = 16384
N_TP = 8


def draw_log_decay(key, part):
    key_sequence_order, key_reach, key_block, key_jitter, key_place, key_keep = jax.random.split(jax.random.fold_in(key, 7), 6)
    order = jax.random.permutation(key_sequence_order, HEADS)
    fast = order < HEADS // 2
    reach = jnp.exp(jax.random.uniform(key_reach, (HEADS,), jnp.float32, math.log(30.0), math.log(100.0)))
    fast_rate = -math.log(10.0) / reach
    slow_rate = jnp.full((HEADS,), -0.1 * math.log(10.0) / SEQ, jnp.float32)
    rate = jnp.where(fast, fast_rate, slow_rate)
    segments = SEQ // TOK_DEV
    factor = jnp.exp(jax.random.uniform(key_block, (HEADS, segments, 1), jnp.float32, math.log(0.5), math.log(2.0)))
    jitter = jnp.exp(jax.random.uniform(key_jitter, (HEADS, segments, TOK_DEV), jnp.float32, -0.5, 0.5))
    per_token_slot = (rate[:, None, None] * factor * jitter).reshape(HEADS, SEQ)
    places = jax.random.randint(key_place, (HEADS, 2), 0, SEQ)
    surviving_items = jax.random.uniform(key_keep, (HEADS, 2), jnp.float32, 0.5, 0.8)
    agreement_count = jnp.arange(SEQ)[None, None, :] == places[:, :, None]
    cluster_bundles = jnp.sum(jnp.where(agreement_count, jnp.log(surviving_items)[:, :, None], 0.0), axis=1)
    return (per_token_slot + cluster_bundles).astype(jnp.float32)


def block_scale(key, dims, cuts, smallest, top_value):
    loudness, own = 1.0, jax.random.fold_in(key, 6)
    for dim, blocks in cuts:
        draws = jnp.exp(jax.random.uniform(jax.random.fold_in(own, dim), (blocks,), jnp.float32, smallest / len(cuts), top_value / len(cuts)))
        loudness = loudness * jnp.repeat(draws, dims[dim] // blocks).reshape([-1 if axis == dim else 1 for axis in range(len(dims))])
    return loudness


def normal_values(rng, dims, scale, limit, pieces=(), held_as=jnp.bfloat16):
    array = scale * jax.random.normal(rng, dims, jnp.float32)
    if pieces:
        array = array * block_scale(rng, dims, pieces, -0.22, 0.18)
    return jnp.clip(array, -limit, limit).astype(held_as)


def setup_inputs(seed: int = 0) -> dict:
    arg_keys = jax.random.split(jax.random.key(seed), 11)
    return {
        "resid": normal_values(arg_keys[0], (SEQ, D), 1.0, 6.0, ((0, 128),)),
        "queries": normal_values(arg_keys[1], (SEQ, HEADS * DK), 1.0, 6.0, ((0, 16), (1, 8))),
        "keys": normal_values(arg_keys[2], (SEQ, HEADS * DK), 1.0, 6.0, ((0, 16), (1, 8))),
        "values": normal_values(arg_keys[3], (SEQ, HEADS * DV), 1.0, 6.0, ((0, 16), (1, 8))),
        "gates": normal_values(arg_keys[4], (SEQ, HEADS * DV), 1.0, 6.0, ((0, 16), (1, 8))),
        "log_decay": draw_log_decay(jax.random.fold_in(arg_keys[10], 71), 0),
        "retention_output_weight": normal_values(arg_keys[6], (HEADS * DV, D), (HEADS * DV // 2) ** -0.5, 0.125, ((0, 8),)),
        "norm_gain": jnp.clip(1.0 + 0.18 * jax.random.normal(arg_keys[7], (D,), jnp.float32), 0.099609375, 1.8984375).astype(jnp.bfloat16),
        "up_weight": normal_values(arg_keys[8], (D, FF), D ** -0.5, 0.125, ((0, 16), (1, 8))),
        "down_weight": normal_values(arg_keys[9], (FF, D), FF ** -0.5, 0.0625, ((0, 8), (1, 16))),
    }


tiny_stabilizer = 1e-06

def round_trip(values_in):
    return lax.optimization_barrier(values_in.astype(jnp.bfloat16)).astype(jnp.float32)

def rotate(values_in, token_indices):
    half_width = values_in.shape[-1] // 2
    inverse = 10000.0 ** (-jnp.arange(0, 2 * half_width, 2, dtype=jnp.float32) / (2 * half_width))
    angles = token_indices[:, None].astype(jnp.float32) * inverse[None, :]
    cosine = jnp.cos(angles)[:, None, :]
    sine_lookup = jnp.sin(angles)[:, None, :]
    first_half = values_in[..., :half_width]
    second = values_in[..., half_width:]
    return jnp.concatenate([first_half * cosine - second * sine_lookup, first_half * sine_lookup + second * cosine], axis=-1)

def normalize(updated, norm_gain):
    widened = updated.astype(jnp.float32)
    scaled = widened * lax.rsqrt(lax.optimization_barrier(jnp.mean(widened * widened, axis=-1, keepdims=True)) + tiny_stabilizer)
    return (scaled * norm_gain.astype(jnp.float32)).astype(jnp.bfloat16)

def block_step(carry_state, per_block):
    query_blk, key_blk, value_blk, gate_blk, cum_blk = per_block
    length = cum_blk.shape[1]
    causal = jnp.arange(length)[:, None] >= jnp.arange(length)[None, :]
    spread = cum_blk[:, :, None] - cum_blk[:, None, :]
    factor = jnp.where(causal[None], jnp.exp(jnp.minimum(spread, 0.0)), 0.0)
    scores = jnp.einsum('ihd,jhd->hij', query_blk, key_blk)
    weights = round_trip(scores * factor)
    within_block = jnp.einsum('hij,jhv->ihv', weights, value_blk)
    decayed = round_trip(query_blk * jnp.exp(cum_blk).T[:, :, None])
    carried_part = jnp.einsum('ihd,hdv->ihv', decayed, round_trip(carry_state))
    retained = within_block + carried_part
    normed = retained * lax.rsqrt(lax.optimization_barrier(jnp.mean(retained * retained, axis=-1, keepdims=True)) + tiny_stabilizer)
    gated_out = (jax.nn.silu(gate_blk) * normed).astype(jnp.bfloat16)
    tile_count_all = cum_blk[:, -1]
    key_decayed = round_trip(key_blk * jnp.exp(tile_count_all[:, None] - cum_blk).T[:, :, None])
    update = jnp.einsum('jhd,jhv->hdv', key_decayed, value_blk)
    return (jnp.exp(tile_count_all)[:, None, None] * carry_state + update, gated_out)

def grouped_product(left, right, groups):
    group_width = left.shape[1] // groups

    def add_group(running, number):
        first_row = (number * group_width).astype(jnp.int32)
        left_part = lax.dynamic_slice_in_dim(left, first_row, group_width, 1)
        right_part = lax.dynamic_slice_in_dim(right, first_row, group_width, 0)
        partial_value = jnp.dot(left_part, right_part, preferred_element_type=jnp.float32)
        return (running + round_trip(partial_value), None)
    running = jnp.zeros((left.shape[0], right.shape[1]), jnp.float32)
    running, unused = lax.scan(add_group, running, jnp.arange(groups, dtype=jnp.int32))
    return running

def channel_mixer(normed, up_weight, down_weight, groups):
    group_width = up_weight.shape[1] // groups

    def add_group(running, number):
        first_row = (number * group_width).astype(jnp.int32)
        up_part = lax.dynamic_slice_in_dim(up_weight, first_row, group_width, 1)
        down_part = lax.dynamic_slice_in_dim(down_weight, first_row, group_width, 0)
        preact = jnp.maximum(jnp.dot(normed, up_part, preferred_element_type=jnp.float32), 0.0)
        hidden = (preact * preact).astype(jnp.bfloat16)
        partial_value = jnp.dot(hidden, down_part, preferred_element_type=jnp.float32)
        return (running + round_trip(partial_value), None)
    running = jnp.zeros((normed.shape[0], down_weight.shape[1]), jnp.float32)
    running, unused = lax.scan(add_group, running, jnp.arange(groups, dtype=jnp.int32))
    return running

def reference(resid, queries, keys, values, gates, log_decay, retention_output_weight, norm_gain, up_weight, down_weight):
    length = queries.shape[0]
    blocks = length // BLOCK
    token_indices = jnp.arange(length, dtype=jnp.int32)
    query_rot = round_trip(rotate(queries.astype(jnp.float32).reshape(length, HEADS, DK), token_indices))
    key_rot = round_trip(rotate(keys.astype(jnp.float32).reshape(length, HEADS, DK), token_indices) * DK ** (-0.5))
    cumulative = jnp.cumsum(log_decay.astype(jnp.float32).reshape(HEADS, blocks, BLOCK), axis=2)
    per_block = (query_rot.reshape(blocks, BLOCK, HEADS, DK), key_rot.reshape(blocks, BLOCK, HEADS, DK), values.astype(jnp.float32).reshape(blocks, BLOCK, HEADS, DV), gates.astype(jnp.float32).reshape(blocks, BLOCK, HEADS, DV), jnp.moveaxis(cumulative, 1, 0))
    unused, gated_out = lax.scan(block_step, jnp.zeros((HEADS, DK, DV), jnp.float32), per_block)
    gated_out = gated_out.reshape(length, HEADS * DV)
    mixed_sum = grouped_product(gated_out, retention_output_weight, N_TP)
    updated = (resid.astype(jnp.float32) + mixed_sum).astype(jnp.bfloat16)
    normed = normalize(updated, norm_gain)
    channel_sum = channel_mixer(normed, up_weight, down_weight, N_TP)
    return (updated.astype(jnp.float32) + channel_sum).astype(jnp.bfloat16)
```

```python
import jax
import jax.numpy as jnp
import numpy as np
from jax import lax
from jax.experimental import pallas as pl
from jax.experimental.pallas import tpu as pltpu
from jax.sharding import Mesh
from jax.sharding import PartitionSpec as P

DK = 256
DV = 512
HALF = DK // 2
BLOCK = 128
BLOCKS = 8
ROWS = 1024
D = 2048
FFL = 1024
QUARTER = DK // 4
EPS = 1e-06
F32 = jnp.float32
BF16 = jnp.bfloat16


def rotation_tables():
    inverse = 10000.0 ** (-np.arange(0, DK, 2, dtype=np.float64) / DK)
    inside = np.arange(BLOCK, dtype=np.float64)[:, None] * inverse[None, :]
    start = (np.arange(128, dtype=np.float64) * BLOCK)[:, None] * inverse[None, :]
    return np.stack([np.cos(inside), np.sin(inside), np.cos(start), np.sin(start)]).astype(np.float32)


class Copies:
    def __init__(self, send, recv):
        self.send, self.recv, self.count, self.made = send, recv, 0, []

    def start(self, src, dst, **where):
        copy = pltpu.make_async_remote_copy(
            src_ref=src,
            dst_ref=dst,
            send_sem=self.send.at[self.count],
            recv_sem=self.recv.at[self.count],
            device_id=where,
            device_id_type=pl.DeviceIdType.MESH,
        )
        copy.start()
        self.count += 1
        self.made.append(copy)
        return copy

    def finish(self):
        for copy in self.made:
            copy.wait_send()


N_COPIES = 64
N_LOCAL = 16


def kernel(
    resid, q_in, k_in, v_in, g_in, ld_in, wo_in, gain_in, up_in, dn_in, tab_in, out,
    q_s, k_s, v_s, g_s, wo_s, resid_s, gain_s, ld_s, tab_s,
    ccol, crow, bstart, s_run, s_blk, local, q_late, gated,
    st_tx, st_rx, in_tx, in_rx, row_tx, row_rx, dec_tx, dec_rx, rdec_tx, rdec_rx,
    p1, p1_rx, ra1_p, ra1_m, rb1_p, rb1_m,
    updated, normed, hidden, up_w, dn_w,
    p2, p2_rx, ra2_p, ra2_m, rb2_p, rb2_m,
    send, recv, loc,
):
    z, y = lax.axis_index("z"), lax.axis_index("y")
    x, c = lax.axis_index("x"), lax.axis_index("c")

    def step(a, by):
        return lax.rem(a + by, 4)

    xp, xm, xo = step(x, 1), step(x, 3), step(x, 2)
    yp, ym = step(y, 1), step(y, 3)
    zp, zm = step(z, 1), step(z, 3)
    other = 1 - c
    net = Copies(send, recv)

    local_copies = []

    def fetch(src, dst):
        copy = pltpu.make_async_copy(src, dst, loc.at[len(local_copies)])
        copy.start()
        local_copies.append(copy)
        return copy

    own_rows = pl.ds(pl.multiple_of((4 * z + y) * 128, 128), 128)
    own_cols = pl.ds(pl.multiple_of((4 * y + z) * 128, 128), 128)

    barrier = pltpu.get_barrier_semaphore()
    for where in (
        {"y": yp}, {"y": ym}, {"y": step(y, 2)},
        {"z": zp}, {"z": zm}, {"z": step(z, 2)},
        {"x": xp}, {"x": xm}, {"c": other},
    ):
        pl.semaphore_signal(barrier, inc=1, device_id=where, device_id_type=pl.DeviceIdType.MESH)

    f_ld = fetch(ld_in, ld_s)
    f_tab = fetch(tab_in, tab_s)
    f_k = fetch(k_in, k_s)
    f_v = fetch(v_in, v_s)
    f_q = fetch(q_in, q_s)
    f_g = fetch(g_in, g_s)
    f_wo = fetch(wo_in, wo_s)
    f_res = fetch(resid, resid_s)
    f_gain = fetch(gain_in, gain_s)
    f_up = fetch(up_in, up_w.at[own_rows, :])
    f_dn = fetch(dn_in, dn_w.at[:, own_cols])

    pl.semaphore_wait(barrier, 9)

    u1p = net.start(up_in, up_w.at[own_rows, :], y=yp)
    u1m = net.start(up_in, up_w.at[own_rows, :], y=ym)
    d1p = net.start(dn_in, dn_w.at[:, own_cols], z=zp)
    d1m = net.start(dn_in, dn_w.at[:, own_cols], z=zm)

    f_ld.wait()
    ii = lax.broadcasted_iota(jnp.int32, (BLOCK, BLOCK), 0)
    jj = lax.broadcasted_iota(jnp.int32, (BLOCK, BLOCK), 1)
    causal = ii >= jj
    lower = jnp.where(causal, 1.0, 0.0).astype(F32)
    ld = ld_s[...]
    nt = (((1,), (1,)), ((), ()))
    by_col = lax.dot_general(lower, ld, nt, precision=lax.Precision.HIGHEST, preferred_element_type=F32)
    crow[...] = lax.dot_general(ld, lower, nt, precision=lax.Precision.HIGHEST, preferred_element_type=F32)
    for n in range(BLOCKS):
        ccol[n * BLOCK : (n + 1) * BLOCK, :] = jnp.broadcast_to(by_col[:, n : n + 1], (BLOCK, 128))

    f_tab.wait()
    f_k.wait()
    f_v.wait()

    def rotated(ref, n):
        rows = pl.ds(pl.multiple_of(n * BLOCK, BLOCK), BLOCK)
        block = (4 * z + y) * BLOCKS + n
        cos_in, sin_in = tab_s[0], tab_s[1]
        cos_at = tab_s[2, pl.ds(block, 1), :]
        sin_at = tab_s[3, pl.ds(block, 1), :]
        cosine = cos_at * cos_in - sin_at * sin_in
        sine = sin_at * cos_in + cos_at * sin_in
        first = ref[rows, 0:HALF].astype(F32)
        second = ref[rows, HALF:DK].astype(F32)
        return rows, first * cosine - second * sine, first * sine + second * cosine

    s_run[...] = jnp.zeros_like(s_run)

    def state_block(n, before):
        rows, a, b = rotated(k_s, n)
        a = (a * DK**-0.5).astype(BF16)
        b = (b * DK**-0.5).astype(BF16)
        k_s[rows, 0:HALF] = a
        k_s[rows, HALF:DK] = b
        total = ccol[pl.ds(n * BLOCK + BLOCK - 1, 1), :]
        to_end = jnp.exp(total - ccol[rows, :])
        decayed = jnp.concatenate(
            [(a.astype(F32) * to_end).astype(BF16), (b.astype(F32) * to_end).astype(BF16)], axis=1
        )
        term = lax.dot_general(
            decayed, v_s[rows, :], (((0,), (0,)), ((), ())), preferred_element_type=F32
        )
        s_blk[n] = s_run[...].astype(BF16)
        s_run[...] = jnp.exp(total[:, 0:1]) * s_run[...] + term
        bstart[pl.ds(n, 1), :] = before
        return before + total

    total = lax.fori_loop(0, BLOCKS, state_block, jnp.zeros((1, 128), F32))

    dec_tx[...] = jnp.broadcast_to(total, (8, 128))
    dec_rx[y] = jnp.broadcast_to(total, (8, 128))
    for part in range(4):
        st_tx[part] = s_run[part * QUARTER : (part + 1) * QUARTER, :].astype(BF16)
    st_copies = []
    for by in (1, 3, 2):
        to = step(y, by)
        st_copies.append(net.start(dec_tx, dec_rx.at[y], y=to))
        st_copies.append(net.start(st_tx.at[to], st_rx.at[y], y=to))
    st_rx[y] = st_tx[y]

    def up_rows(zz, yy, first, size):
        return pl.ds(pl.multiple_of(zz * 512 + yy * 128 + first, 64), size)

    def dn_cols(yy, zz):
        return pl.ds(pl.multiple_of(yy * 512 + zz * 128, 128), 128)

    u1p.wait_recv()
    here = up_w.at[up_rows(z, ym, 0, 64), :]
    u1fp = net.start(here, here, y=yp)
    u1m.wait_recv()
    here = up_w.at[up_rows(z, yp, 64, 64), :]
    u1fm = net.start(here, here, y=ym)
    d1p.wait_recv()
    here = dn_w.at[0:512, dn_cols(y, zm)]
    d1fp = net.start(here, here, z=zp)
    d1m.wait_recv()
    here = dn_w.at[512:1024, dn_cols(y, zp)]
    d1fm = net.start(here, here, z=zm)

    f_q.wait()
    f_g.wait()

    def local_block(n, carry):
        rows, a, b = rotated(q_s, n)
        col = ccol[rows, :]
        a = a.astype(BF16)
        b = b.astype(BF16)
        query = jnp.concatenate([a, b], axis=1)
        scores = lax.dot_general(query, k_s[rows, :], nt, preferred_element_type=F32)
        spread = col - crow[pl.ds(n, 1), :]
        factor = jnp.where(causal, jnp.exp(jnp.minimum(spread, 0.0)), 0.0)
        weights = (scores * factor).astype(BF16)
        a = a.astype(F32)
        b = b.astype(F32)
        early = jnp.exp(col)
        decayed = jnp.concatenate([(a * early).astype(BF16), (b * early).astype(BF16)], axis=1)
        late = jnp.exp(col + bstart[pl.ds(n, 1), :])
        q_late[rows, 0:HALF] = (a * late).astype(BF16)
        q_late[rows, HALF:DK] = (b * late).astype(BF16)
        local[rows, :] = jnp.dot(
            weights, v_s[rows, :], preferred_element_type=F32
        ) + jnp.dot(decayed, s_blk[n], preferred_element_type=F32)
        return carry

    lax.fori_loop(0, 4, local_block, 0)

    for copy in st_copies:
        copy.wait_recv()
    run = st_rx[0].astype(F32)
    log_row = dec_rx[0]
    for at in range(1, 4):
        run = jnp.exp(dec_rx[at][0:1, 0:1]) * run + st_rx[at].astype(F32)
        log_row = log_row + dec_rx[at]
    row_tx[...] = run.astype(BF16)
    row_rx[z] = run.astype(BF16)
    rdec_tx[...] = log_row
    rdec_rx[z] = log_row
    row_copies = []
    for by in (1, 3, 2):
        to = step(z, by)
        row_copies.append(net.start(rdec_tx, rdec_rx.at[z], z=to))
        row_copies.append(net.start(row_tx, row_rx.at[z], z=to))

    lax.fori_loop(4, 8, local_block, 0)

    for copy in row_copies:
        copy.wait_recv()
    run = jnp.zeros((QUARTER, DV), F32)
    for at in range(4):
        later = jnp.exp(rdec_rx[at][0:1, 0:1]) * run + row_rx[at].astype(F32)
        run = jnp.where(at < z, later, run)
    for at in range(4):
        in_tx[at] = run.astype(BF16)
        if at < 3:
            run = jnp.exp(dec_rx[at][0:1, 0:1]) * run + st_rx[at].astype(F32)
    in_copies = []
    for by in (1, 3, 2):
        to = step(y, by)
        in_copies.append(net.start(in_tx.at[to], in_rx.at[y], y=to))
    in_rx[y] = in_tx[y]

    u1fp.wait_recv()
    u1fm.wait_recv()
    d1fp.wait_recv()
    d1fm.wait_recv()
    f_up.wait()
    f_dn.wait()

    def up_half(zz, half):
        return up_w.at[pl.ds(pl.multiple_of(zz * 512 + half * 256, 256), 256), :]

    def dn_half(yy, half):
        return dn_w.at[half * 512 : (half + 1) * 512, pl.ds(pl.multiple_of(yy * 512, 512), 512)]

    u2p = net.start(up_half(z, 0), up_half(z, 0), z=zp)
    u2m = net.start(up_half(z, 1), up_half(z, 1), z=zm)
    d2p = net.start(dn_half(y, 0), dn_half(y, 0), y=yp)
    d2m = net.start(dn_half(y, 1), dn_half(y, 1), y=ym)
    u3p = net.start(up_half(z, 1), up_half(z, 1), z=zp)
    u3m = net.start(up_half(z, 0), up_half(z, 0), z=zm)
    d3p = net.start(dn_half(y, 1), dn_half(y, 1), y=yp)
    d3m = net.start(dn_half(y, 0), dn_half(y, 0), y=ym)

    f_wo.wait()
    f_res.wait()
    f_gain.wait()
    for copy in in_copies:
        copy.wait_recv()

    def gate_rows(d):
        def part(i, carry):
            rows = pl.ds(pl.multiple_of(d * 256 + i * 128, 128), 128)
            incoming = jnp.concatenate([in_rx[at] for at in range(4)], axis=0)
            kept = local[rows, :] + jnp.dot(q_late[rows, :], incoming, preferred_element_type=F32)
            scale = lax.rsqrt(jnp.mean(kept * kept, axis=-1, keepdims=True) + EPS)
            gate = g_s[rows, :].astype(F32)
            gate = gate / (1.0 + jnp.exp(-gate))
            gated[pl.ds(pl.multiple_of(i * 128, 128), 128), :] = (gate * kept * scale).astype(BF16)
            return carry

        lax.fori_loop(0, 2, part, 0)

    def project(d):
        gate_rows(d)
        for j in range(4):
            part = jnp.dot(
                gated[...], wo_s[:, j * 512 : (j + 1) * 512], preferred_element_type=F32
            ).astype(BF16)
            to = slice((j % 2) * 512, (j % 2) * 512 + 512)
            p1[d, 0, j // 2, :, to] = part[0:128]
            p1[d, 1, j // 2, :, to] = part[128:256]

    def accumulate(p, d, half, extra):
        p[d, c, half] = (p[d, c, half].astype(F32) + extra[...].astype(F32)).astype(BF16)

    def pair(p, p_rx, d):
        return net.start(p.at[d, other], p_rx.at[d], c=other)

    def pair_sum(copy, p, p_rx, d):
        copy.wait_recv()
        for half in range(2):
            accumulate(p, d, half, p_rx.at[d, half])

    project(xo)
    w_o = pair(p1, p1_rx, xo)
    project(xp)
    w_p = pair(p1, p1_rx, xp)
    pair_sum(w_o, p1, p1_rx, xo)
    a_p = net.start(p1.at[xo, c, 0], ra1_p, x=xp)
    a_m = net.start(p1.at[xo, c, 1], ra1_m, x=xm)
    project(xm)
    w_m = pair(p1, p1_rx, xm)
    pair_sum(w_p, p1, p1_rx, xp)
    b_p = net.start(p1.at[xp, c, 1], rb1_p.at[1], x=xp)
    project(x)
    w_s = pair(p1, p1_rx, x)
    pair_sum(w_m, p1, p1_rx, xm)
    b_m = net.start(p1.at[xm, c, 0], rb1_m.at[0], x=xm)
    a_p.wait_recv()
    accumulate(p1, xp, 0, ra1_p)
    c_p = net.start(p1.at[xp, c, 0], rb1_p.at[0], x=xp)
    a_m.wait_recv()
    accumulate(p1, xm, 1, ra1_m)
    c_m = net.start(p1.at[xm, c, 1], rb1_m.at[1], x=xm)
    w_s.wait_recv()

    u2p.wait_recv()
    u2fp = net.start(up_half(zm, 0), up_half(zm, 0), z=zp)
    u2m.wait_recv()
    u2fm = net.start(up_half(zp, 1), up_half(zp, 1), z=zm)
    d2p.wait_recv()
    d2fp = net.start(dn_half(ym, 0), dn_half(ym, 0), y=yp)
    d2m.wait_recv()
    d2fm = net.start(dn_half(yp, 1), dn_half(yp, 1), y=ym)

    for copy in (b_p, b_m, c_p, c_m):
        copy.wait_recv()

    def norm_rows(i, carry):
        rows = pl.ds(pl.multiple_of(i * 32, 32), 32)
        halves = []
        for half in range(2):
            cols = slice(half * 1024, (half + 1) * 1024)
            value = p1[x, c, half, rows, :].astype(F32) + p1_rx[x, half, rows, :].astype(F32)
            value = value + (rb1_p[half, rows, :].astype(F32) + rb1_m[half, rows, :].astype(F32))
            value = (resid_s[rows, cols].astype(F32) + value).astype(BF16)
            updated[rows, cols] = value
            halves.append(value.astype(F32))
        square = sum(jnp.sum(v * v, axis=-1, keepdims=True) for v in halves)
        scale = lax.rsqrt(square * (1.0 / D) + EPS)
        for half in range(2):
            cols = slice(half * 1024, (half + 1) * 1024)
            normed[x, c, rows, cols] = (halves[half] * scale * gain_s[:, cols]).astype(BF16)
        return carry

    lax.fori_loop(0, 4, norm_rows, 0)

    own = normed.at[x, c]
    n_c = net.start(own, own, c=other)
    n_p = net.start(own, own, x=xp)
    n_m = net.start(own, own, x=xm)

    for copy in (u3p, u3m, d3p, d3m, u2fp, u2fm, d2fp, d2fm):
        copy.wait_recv()

    def mix(d):
        rows = normed[d].reshape(256, D)
        for j in range(2):
            cols = slice(j * 512, (j + 1) * 512)
            pre = jnp.maximum(jnp.dot(rows, up_w[:, cols], preferred_element_type=F32), 0.0)
            hidden[:, cols] = (pre * pre).astype(BF16)
        for yy in range(4):
            part = jnp.dot(
                hidden[...], dn_w[:, yy * 512 : (yy + 1) * 512], preferred_element_type=F32
            ).astype(BF16)
            for zz in range(4):
                to = slice(((zz % 2) * 4 + yy) * 128, ((zz % 2) * 4 + yy) * 128 + 128)
                piece = part[:, zz * 128 : (zz + 1) * 128]
                p2[d, 0, zz // 2, :, to] = piece[0:128]
                p2[d, 1, zz // 2, :, to] = piece[128:256]

    n_c.wait_recv()
    mix(x)
    w_s = pair(p2, p2_rx, x)
    n_p.wait_recv()
    came = normed.at[xm, c]
    half_row = normed.at[xm, c, 0:64, :]
    n_fp = net.start(half_row, half_row, x=xp)
    n_cm = net.start(came, came, c=other)
    n_m.wait_recv()
    came = normed.at[xp, c]
    half_row = normed.at[xp, c, 64:128, :]
    n_fm = net.start(half_row, half_row, x=xm)
    n_cp = net.start(came, came, c=other)
    n_cp.wait_recv()
    mix(xp)
    w_p = pair(p2, p2_rx, xp)
    n_fp.wait_recv()
    here = normed.at[xo, c, 0:64, :]
    n_c0 = net.start(here, here, c=other)
    n_fm.wait_recv()
    here = normed.at[xo, c, 64:128, :]
    n_c1 = net.start(here, here, c=other)
    pair_sum(w_p, p2, p2_rx, xp)
    b_p = net.start(p2.at[xp, c, 1], rb2_p.at[1], x=xp)
    n_cm.wait_recv()
    mix(xm)
    w_m = pair(p2, p2_rx, xm)
    n_c0.wait_recv()
    n_c1.wait_recv()
    pair_sum(w_m, p2, p2_rx, xm)
    b_m = net.start(p2.at[xm, c, 0], rb2_m.at[0], x=xm)
    mix(xo)
    w_o = pair(p2, p2_rx, xo)
    pair_sum(w_o, p2, p2_rx, xo)
    a_p = net.start(p2.at[xo, c, 0], ra2_p, x=xp)
    a_m = net.start(p2.at[xo, c, 1], ra2_m, x=xm)
    w_s.wait_recv()
    a_p.wait_recv()
    accumulate(p2, xp, 0, ra2_p)
    c_p = net.start(p2.at[xp, c, 0], rb2_p.at[0], x=xp)
    a_m.wait_recv()
    accumulate(p2, xm, 1, ra2_m)
    c_m = net.start(p2.at[xm, c, 1], rb2_m.at[1], x=xm)
    for copy in (b_p, b_m, c_p, c_m):
        copy.wait_recv()

    def final_rows(i, carry):
        rows = pl.ds(pl.multiple_of(i * 32, 32), 32)
        for half in range(2):
            cols = slice(half * 1024, (half + 1) * 1024)
            value = p2[x, c, half, rows, :].astype(F32) + p2_rx[x, half, rows, :].astype(F32)
            value = value + (rb2_p[half, rows, :].astype(F32) + rb2_m[half, rows, :].astype(F32))
            out[rows, cols] = (updated[rows, cols].astype(F32) + value).astype(BF16)
        return carry

    lax.fori_loop(0, 4, final_rows, 0)
    net.finish()


def body(resid, q, k, v, g, log_decay, wo, gain, up, dn):
    vm = pltpu.VMEM
    scratch = [
        vm((ROWS, DK), BF16), vm((ROWS, DK), BF16), vm((ROWS, DV), BF16), vm((ROWS, DV), BF16),
        vm((DV, D), BF16), vm((128, D), BF16), vm((1, D), F32), vm((BLOCKS, 128), F32),
        vm((4, 128, 128), F32),
        vm((ROWS, 128), F32), vm((BLOCKS, 128), F32), vm((BLOCKS, 128), F32),
        vm((DK, DV), F32), vm((BLOCKS, DK, DV), BF16), vm((ROWS, DV), F32), vm((ROWS, DK), BF16),
        vm((256, DV), BF16),
        vm((4, QUARTER, DV), BF16), vm((4, QUARTER, DV), BF16),
        vm((4, QUARTER, DV), BF16), vm((4, QUARTER, DV), BF16),
        vm((QUARTER, DV), BF16), vm((4, QUARTER, DV), BF16),
        vm((8, 128), F32), vm((4, 8, 128), F32), vm((8, 128), F32), vm((4, 8, 128), F32),
        vm((4, 2, 2, 128, 1024), BF16), vm((4, 2, 128, 1024), BF16),
        vm((128, 1024), BF16), vm((128, 1024), BF16),
        vm((2, 128, 1024), BF16), vm((2, 128, 1024), BF16),
        vm((128, D), BF16), vm((4, 2, 128, D), BF16), vm((256, FFL), BF16),
        vm((D, FFL), BF16), vm((FFL, D), BF16),
        vm((4, 2, 2, 128, 1024), BF16), vm((4, 2, 128, 1024), BF16),
        vm((128, 1024), BF16), vm((128, 1024), BF16),
        vm((2, 128, 1024), BF16), vm((2, 128, 1024), BF16),
        pltpu.SemaphoreType.DMA((N_COPIES,)),
        pltpu.SemaphoreType.DMA((N_COPIES,)),
        pltpu.SemaphoreType.DMA((N_LOCAL,)),
    ]
    anywhere = pl.BlockSpec(memory_space=pl.ANY)
    return pl.pallas_call(
        kernel,
        out_shape=jax.ShapeDtypeStruct((128, D), BF16),
        in_specs=[anywhere] * 11,
        out_specs=pl.BlockSpec(memory_space=pltpu.VMEM),
        scratch_shapes=scratch,
        compiler_params=pltpu.CompilerParams(
            collective_id=0, has_side_effects=True, vmem_limit_bytes=66_000_000
        ),
    )(
        resid, q, k, v, g, log_decay.reshape(BLOCKS, BLOCK), wo,
        gain.astype(F32).reshape(1, D), up, dn, jnp.asarray(rotation_tables()),
    )


def solution(mesh):
    torus = Mesh(mesh.devices.reshape(4, 4, 4, 2), ("z", "y", "x", "c"))
    sp, tp = ("z", "y"), ("x", "c")
    placed = (
        P(("z", "y", "x", "c"), None),
        P(sp, tp),
        P(sp, tp),
        P(sp, tp),
        P(sp, tp),
        P(tp, sp),
        P(tp, None),
        P(),
        P(sp, tp),
        P(tp, sp),
    )
    return jax.shard_map(
        body, mesh=torus, in_specs=placed, out_specs=P(("z", "y", "x", "c"), None), check_vma=False
    )
```

```python
import jax
import jax.numpy as jnp
import numpy as np
from jax import lax
from jax.experimental import pallas as pl
from jax.experimental.pallas import tpu as pltpu
from jax.sharding import Mesh
from jax.sharding import PartitionSpec as P

DK = 256
DV = 512
HALF = DK // 2
BLOCK = 128
BLOCKS = 8
ROWS = 1024
D = 2048
FFL = 1024
QUARTER = DK // 4
EPS = 1e-06
F32 = jnp.float32
BF16 = jnp.bfloat16


def rotation_tables():
    inverse = 10000.0 ** (-np.arange(0, DK, 2, dtype=np.float64) / DK)
    inside = np.arange(BLOCK, dtype=np.float64)[:, None] * inverse[None, :]
    start = (np.arange(128, dtype=np.float64) * BLOCK)[:, None] * inverse[None, :]
    return np.stack([np.cos(inside), np.sin(inside), np.cos(start), np.sin(start)]).astype(np.float32)


class Phases:
    def __init__(self):
        self.scope = None

    def __call__(self, name):
        if self.scope is not None:
            self.scope.__exit__(None, None, None)
        self.scope = None
        if name is not None:
            self.scope = jax.named_scope(name)
            self.scope.__enter__()


class Copies:
    def __init__(self, send, recv):
        self.send, self.recv, self.count, self.made = send, recv, 0, []

    def start(self, src, dst, **where):
        copy = pltpu.make_async_remote_copy(
            src_ref=src,
            dst_ref=dst,
            send_sem=self.send.at[self.count],
            recv_sem=self.recv.at[self.count],
            device_id=where,
            device_id_type=pl.DeviceIdType.MESH,
        )
        copy.start()
        self.count += 1
        self.made.append(copy)
        return copy

    def finish(self):
        for copy in self.made:
            copy.wait_send()


N_COPIES = 128
N_LOCAL = 16


def kernel(
    resid, q_in, k_in, v_in, g_in, ld_in, wo_in, gain_in, up_in, dn_in, tab_in, out,
    q_s, k_s, v_s, g_s, wo_s, resid_s, gain_s, ld_s, tab_s,
    ccol, crow, bstart, s_run, s_blk, local, q_late, gated, gate_f,
    st_tx, st_rx, in_tx, in_rx, row_tx, row_rx, dec_tx, dec_rx, rdec_tx, rdec_rx,
    p1, p1_rx, ra1_p, ra1_m, rb1_p, rb1_m,
    updated, normed, hidden, up_w, dn_w,
    p2, p2_rx, ra2_p, ra2_m, rb2_p, rb2_m, out_s,
    send, recv, loc,
):
    z, y = lax.axis_index("z"), lax.axis_index("y")
    x, c = lax.axis_index("x"), lax.axis_index("c")

    def step(a, by):
        return lax.rem(a + by, 4)

    xp, xm, xo = step(x, 1), step(x, 3), step(x, 2)
    yp, ym = step(y, 1), step(y, 3)
    zp, zm = step(z, 1), step(z, 3)
    other = 1 - c
    net = Copies(send, recv)
    phase = Phases()
    phase("s00_barrier")

    local_copies = []

    def fetch(src, dst):
        copy = pltpu.make_async_copy(src, dst, loc.at[len(local_copies)])
        copy.start()
        local_copies.append(copy)
        return copy

    own_rows = pl.ds(pl.multiple_of((4 * z + y) * 128, 128), 128)
    own_cols = pl.ds(pl.multiple_of((4 * y + z) * 128, 128), 128)

    barrier = pltpu.get_barrier_semaphore()
    for where in (
        {"y": yp}, {"y": ym}, {"y": step(y, 2)},
        {"z": zp}, {"z": zm}, {"z": step(z, 2)},
        {"x": xp}, {"x": xm}, {"c": other},
    ):
        pl.semaphore_signal(barrier, inc=1, device_id=where, device_id_type=pl.DeviceIdType.MESH)

    f_ld = fetch(ld_in, ld_s)
    f_tab = fetch(tab_in, tab_s)
    f_k = fetch(k_in, k_s)
    f_v = fetch(v_in, v_s)
    f_q = fetch(q_in, q_s)
    f_g = fetch(g_in, g_s)
    f_wo = fetch(wo_in, wo_s)
    f_res = fetch(resid, resid_s)
    f_gain = fetch(gain_in, gain_s)
    f_up = fetch(up_in, up_w.at[own_rows, :])
    f_dn = fetch(dn_in, dn_w.at[:, own_cols])

    phase("s01_decays")
    f_ld.wait()
    ii = lax.broadcasted_iota(jnp.int32, (BLOCK, BLOCK), 0)
    jj = lax.broadcasted_iota(jnp.int32, (BLOCK, BLOCK), 1)
    causal = ii >= jj
    lower = jnp.where(causal, 1.0, 0.0).astype(F32)
    ld = ld_s[...]
    nt = (((1,), (1,)), ((), ()))
    by_col = lax.dot_general(lower, ld, nt, precision=lax.Precision.HIGHEST, preferred_element_type=F32)
    crow[...] = lax.dot_general(ld, lower, nt, precision=lax.Precision.HIGHEST, preferred_element_type=F32)
    for n in range(BLOCKS):
        ccol[n * BLOCK : (n + 1) * BLOCK, :] = jnp.broadcast_to(by_col[:, n : n + 1], (BLOCK, 128))

    phase("s02_kvwait")
    f_tab.wait()
    f_k.wait()
    f_v.wait()

    def rotated(ref, n):
        rows = pl.ds(pl.multiple_of(n * BLOCK, BLOCK), BLOCK)
        block = (4 * z + y) * BLOCKS + n
        cos_in, sin_in = tab_s[0], tab_s[1]
        cos_at = tab_s[2, pl.ds(block, 1), :]
        sin_at = tab_s[3, pl.ds(block, 1), :]
        cosine = cos_at * cos_in - sin_at * sin_in
        sine = sin_at * cos_in + cos_at * sin_in
        first = ref[rows, 0:HALF].astype(F32)
        second = ref[rows, HALF:DK].astype(F32)
        return rows, first * cosine - second * sine, first * sine + second * cosine

    phase("s03_states")
    s_run[...] = jnp.zeros_like(s_run)

    def state_block(n, before):
        rows, a, b = rotated(k_s, n)
        a = (a * DK**-0.5).astype(BF16)
        b = (b * DK**-0.5).astype(BF16)
        k_s[rows, 0:HALF] = a
        k_s[rows, HALF:DK] = b
        total = ccol[pl.ds(n * BLOCK + BLOCK - 1, 1), :]
        to_end = jnp.exp(total - ccol[rows, :])
        decayed = jnp.concatenate(
            [(a.astype(F32) * to_end).astype(BF16), (b.astype(F32) * to_end).astype(BF16)], axis=1
        )
        term = lax.dot_general(
            decayed, v_s[rows, :], (((0,), (0,)), ((), ())), preferred_element_type=F32
        )
        s_blk[n] = s_run[...].astype(BF16)
        s_run[...] = jnp.exp(total[:, 0:1]) * s_run[...] + term
        bstart[pl.ds(n, 1), :] = before
        return before + total

    total = lax.fori_loop(0, 4, state_block, jnp.zeros((1, 128), F32))
    phase("s03b_barrier")
    pl.semaphore_wait(barrier, 9)

    def up_at(zz, yy, half=None):
        first, size = (0, 128) if half is None else (half * 64, 64)
        return up_w.at[pl.ds(pl.multiple_of(zz * 512 + yy * 128 + first, 64), size), :]

    def dn_at(yy, zz, half=None):
        cols = pl.ds(pl.multiple_of(yy * 512 + zz * 128, 128), 128)
        return dn_w.at[:, cols] if half is None else dn_w.at[half * 512 : half * 512 + 512, cols]

    def up_own(half):
        return up_in.at[half * 64 : half * 64 + 64, :]

    def dn_own(half):
        return dn_in.at[half * 512 : half * 512 + 512, :]

    d1a = (
        net.start(dn_own(0), dn_at(y, z, 0), z=zp),
        net.start(dn_own(1), dn_at(y, z, 1), z=zm),
    )
    d1b = (
        net.start(dn_own(1), dn_at(y, z, 1), z=zp),
        net.start(dn_own(0), dn_at(y, z, 0), z=zm),
    )
    phase("s03c_states")
    total = lax.fori_loop(4, BLOCKS, state_block, total)

    phase("s04_sendstate")
    dec_tx[...] = jnp.broadcast_to(total, (8, 128))
    dec_rx[y] = jnp.broadcast_to(total, (8, 128))
    for part in range(4):
        st_tx[part] = s_run[part * QUARTER : (part + 1) * QUARTER, :].astype(BF16)
    st_copies = []
    for by in (1, 3, 2):
        to = step(y, by)
        st_copies.append(net.start(dec_tx, dec_rx.at[y], y=to))
        st_copies.append(net.start(st_tx.at[to], st_rx.at[y], y=to))
    st_rx[y] = st_tx[y]

    u1a = (
        net.start(up_own(0), up_at(z, y, 0), y=yp),
        net.start(up_own(1), up_at(z, y, 1), y=ym),
    )
    u1b = (
        net.start(up_own(1), up_at(z, y, 1), y=yp),
        net.start(up_own(0), up_at(z, y, 0), y=ym),
    )
    def arrived(*groups):
        for group in groups:
            for copy in group:
                copy.wait_recv()

    def up_out(yy):
        return (net.start(up_at(z, yy), up_at(z, yy), z=zp), net.start(up_at(z, yy), up_at(z, yy), z=zm))

    def dn_out(zz):
        return (net.start(dn_at(y, zz), dn_at(y, zz), y=yp), net.start(dn_at(y, zz), dn_at(y, zz), y=ym))

    def up_on(yy):
        return (
            net.start(up_at(zm, yy, 0), up_at(zm, yy, 0), z=zp),
            net.start(up_at(zp, yy, 1), up_at(zp, yy, 1), z=zm),
        )

    def dn_on(zz):
        return (
            net.start(dn_at(ym, zz, 0), dn_at(ym, zz, 0), y=yp),
            net.start(dn_at(yp, zz, 1), dn_at(yp, zz, 1), y=ym),
        )

    phase("s06_local1")
    f_q.wait()
    f_g.wait()

    def local_block(n, carry):
        rows, a, b = rotated(q_s, n)
        col = ccol[rows, :]
        a = a.astype(BF16)
        b = b.astype(BF16)
        query = jnp.concatenate([a, b], axis=1)
        scores = lax.dot_general(query, k_s[rows, :], nt, preferred_element_type=F32)
        spread = col - crow[pl.ds(n, 1), :]
        factor = jnp.where(causal, jnp.exp(jnp.minimum(spread, 0.0)), 0.0)
        weights = (scores * factor).astype(BF16)
        a = a.astype(F32)
        b = b.astype(F32)
        early = jnp.exp(col)
        decayed = jnp.concatenate([(a * early).astype(BF16), (b * early).astype(BF16)], axis=1)
        late = jnp.exp(col + bstart[pl.ds(n, 1), :])
        q_late[rows, 0:HALF] = (a * late).astype(BF16)
        q_late[rows, HALF:DK] = (b * late).astype(BF16)
        local[rows, :] = jnp.dot(
            weights, v_s[rows, :], preferred_element_type=F32
        ) + jnp.dot(decayed, s_blk[n], preferred_element_type=F32)
        return carry

    lax.fori_loop(0, 4, local_block, 0)

    def gate_block(n, carry):
        rows = pl.ds(pl.multiple_of(n * 64, 64), 64)
        gate = g_s[rows, :].astype(F32)
        gate_f[rows, :] = gate / (1.0 + jnp.exp(-gate))
        return carry

    lax.fori_loop(0, 16, gate_block, 0)

    phase("s07_waitstate")
    for copy in st_copies:
        copy.wait_recv()
    phase("s08_rowtotal")
    run = st_rx[0].astype(F32)
    log_row = dec_rx[0]
    for at in range(1, 4):
        run = jnp.exp(dec_rx[at][0:1, 0:1]) * run + st_rx[at].astype(F32)
        log_row = log_row + dec_rx[at]
    row_tx[...] = run.astype(BF16)
    row_rx[z] = run.astype(BF16)
    rdec_tx[...] = log_row
    rdec_rx[z] = log_row
    row_copies = []
    for by in (1, 3, 2):
        to = step(z, by)
        row_copies.append(net.start(rdec_tx, rdec_rx.at[z], z=to))
        row_copies.append(net.start(row_tx, row_rx.at[z], z=to))

    phase("s09b_w")
    arrived(d1a)
    d1c = (
        net.start(dn_at(y, zm, 0), dn_at(y, zm, 0), z=zp),
        net.start(dn_at(y, zp, 1), dn_at(y, zp, 1), z=zm),
    )
    f_up.wait()
    u2_own = up_out(y)
    phase("s09_local2")
    lax.fori_loop(4, 8, local_block, 0)
    phase("s10_waitrow")

    for copy in row_copies:
        copy.wait_recv()
    phase("s11_incoming")
    run = jnp.zeros((QUARTER, DV), F32)
    for at in range(4):
        later = jnp.exp(rdec_rx[at][0:1, 0:1]) * run + row_rx[at].astype(F32)
        run = jnp.where(at < z, later, run)
    for at in range(4):
        in_tx[at] = run.astype(BF16)
        if at < 3:
            run = jnp.exp(dec_rx[at][0:1, 0:1]) * run + st_rx[at].astype(F32)
    in_copies = []
    for by in (1, 3, 2):
        to = step(y, by)
        in_copies.append(net.start(in_tx.at[to], in_rx.at[y], y=to))
    in_rx[y] = in_tx[y]

    phase("s12_w2wait")
    arrived(u1a)
    u1c = (
        net.start(up_at(z, ym, 0), up_at(z, ym, 0), y=yp),
        net.start(up_at(z, yp, 1), up_at(z, yp, 1), y=ym),
    )
    f_dn.wait()
    d2_own = dn_out(z)
    arrived(u1b, d1b)
    u2_m, u2_p = up_out(ym), up_out(yp)
    d2_m, d2_p = dn_out(zm), dn_out(zp)

    phase("s13_waitin")
    f_wo.wait()
    f_res.wait()
    f_gain.wait()
    for copy in in_copies:
        copy.wait_recv()

    def chunk(h):
        return slice(h * 64, h * 64 + 64)

    def project(d, h):
        picks = [pl.ds(pl.multiple_of(d * 256 + i * 128 + h * 64, 64), 64) for i in range(2)]

        def both(ref):
            return jnp.concatenate([ref[rows, :] for rows in picks], axis=0)

        incoming = jnp.concatenate([in_rx[at] for at in range(4)], axis=0)
        kept = both(local) + jnp.dot(both(q_late), incoming, preferred_element_type=F32)
        scale = lax.rsqrt(jnp.mean(kept * kept, axis=-1, keepdims=True) + EPS)
        gated[...] = (both(gate_f) * kept * scale).astype(BF16)
        for j in range(4):
            part = jnp.dot(
                gated[...], wo_s[:, j * 512 : (j + 1) * 512], preferred_element_type=F32
            ).astype(BF16)
            to = slice((j % 2) * 512, (j % 2) * 512 + 512)
            p1[d, 0, j // 2, chunk(h), to] = part[0:64]
            p1[d, 1, j // 2, chunk(h), to] = part[64:128]

    def mix(d, h):
        rows = normed[d, :, chunk(h), :].reshape(128, D)
        for j in range(2):
            cols = slice(j * 512, (j + 1) * 512)
            pre = jnp.maximum(jnp.dot(rows, up_w[:, cols], preferred_element_type=F32), 0.0)
            hidden[:, cols] = (pre * pre).astype(BF16)
        for yy in range(4):
            part = jnp.dot(
                hidden[...], dn_w[:, yy * 512 : (yy + 1) * 512], preferred_element_type=F32
            ).astype(BF16)
            for zz in range(4):
                to = slice(((zz % 2) * 4 + yy) * 128, ((zz % 2) * 4 + yy) * 128 + 128)
                piece = part[:, zz * 128 : (zz + 1) * 128]
                p2[d, 0, zz // 2, chunk(h), to] = piece[0:64]
                p2[d, 1, zz // 2, chunk(h), to] = piece[64:128]

    def ring_sum(name, compute, p, p_rx, ra_p, ra_m, rb_p, rb_m):
        pairs = {}

        def add(d, h, half, extra):
            p[d, c, half, chunk(h), :] = (p[d, c, half, chunk(h), :].astype(F32) + extra.astype(F32)).astype(BF16)

        def work(key, d, h):
            phase(f"{name}{h}_work_{key}")
            compute(d, h)
            pairs[key, h] = net.start(p.at[d, other, :, chunk(h), :], p_rx.at[d, :, chunk(h), :], c=other)
            phase(f"{name}{h}_after_{key}")

        def pair_sum(key, d, h):
            phase(f"{name}{h}_pair_{key}")
            pairs[key, h].wait_recv()
            for half in range(2):
                add(d, h, half, p_rx[d, half, chunk(h), :])

        def piece(d, h, half):
            return p.at[d, c, half, chunk(h), :]

        a_copies, b_copies, c_copies = {}, {}, {}

        def send_a(h):
            a_copies[h] = (
                net.start(piece(xo, h, 0), ra_p.at[h], x=xp),
                net.start(piece(xo, h, 1), ra_m.at[h], x=xm),
            )

        def send_b(h, plus):
            if plus:
                copy = net.start(piece(xp, h, 1), rb_p.at[h, 1], x=xp)
            else:
                copy = net.start(piece(xm, h, 0), rb_m.at[h, 0], x=xm)
            b_copies[h, plus] = copy

        def send_c(h):
            phase(f"{name}{h}_wait_a")
            plus, minus = a_copies[h]
            plus.wait_recv()
            add(xp, h, 0, ra_p[h])
            first = net.start(piece(xp, h, 0), rb_p.at[h, 0], x=xp)
            minus.wait_recv()
            add(xm, h, 1, ra_m[h])
            c_copies[h] = (first, net.start(piece(xm, h, 1), rb_m.at[h, 1], x=xm))

        def complete(h):
            phase(f"{name}{h}_wait_bc")
            pairs["x", h].wait_recv()
            for copy in (b_copies[h, True], b_copies[h, False], *c_copies[h]):
                copy.wait_recv()

        work("xo", xo, 0)
        work("xp", xp, 0)
        pair_sum("xo", xo, 0)
        send_a(0)
        work("xm", xm, 0)
        pair_sum("xp", xp, 0)
        send_b(0, True)
        yield
        work("x", x, 0)
        pair_sum("xm", xm, 0)
        send_b(0, False)
        yield
        work("xo", xo, 1)
        work("xp", xp, 1)
        pair_sum("xo", xo, 1)
        send_a(1)
        work("xm", xm, 1)
        pair_sum("xp", xp, 1)
        work("x", x, 1)
        pair_sum("xm", xm, 1)
        yield
        send_c(0)
        send_b(1, True)
        send_b(1, False)
        yield
        send_c(1)
        yield
        complete(0)
        yield
        complete(1)
        yield

    def total_of(p, p_rx, rb_p, rb_m, h, half, first, size):
        rows = slice(h * 64 + first, h * 64 + first + size)
        near = slice(first, first + size)
        value = p[x, c, half, rows, :].astype(F32) + p_rx[x, half, rows, :].astype(F32)
        return value + (rb_p[h, half, near, :].astype(F32) + rb_m[h, half, near, :].astype(F32))

    def norm_chunk(h):
        phase(f"n{h}_norm")
        for first in range(0, 64, 32):
            rows = slice(h * 64 + first, h * 64 + first + 32)
            halves = []
            for half in range(2):
                cols = slice(half * 1024, (half + 1) * 1024)
                value = total_of(p1, p1_rx, rb1_p, rb1_m, h, half, first, 32)
                value = (resid_s[rows, cols].astype(F32) + value).astype(BF16)
                updated[rows, cols] = value
                halves.append(value.astype(F32))
            square = sum(jnp.sum(v * v, axis=-1, keepdims=True) for v in halves)
            scale = lax.rsqrt(square * (1.0 / D) + EPS)
            for half in range(2):
                cols = slice(half * 1024, (half + 1) * 1024)
                normed[x, c, rows, cols] = (halves[half] * scale * gain_s[:, cols]).astype(BF16)

    def share(d, first, size, **where):
        here = normed.at[d, c, first : first + size, :]
        return net.start(here, here, **where)

    def first_out(h):
        return (share(x, h * 64, 32, x=xp), share(x, h * 64 + 32, 32, x=xm))

    def rest_out(h):
        return (share(x, h * 64 + 32, 32, x=xp), share(x, h * 64, 32, x=xm))

    def pass_on(h):
        return (share(xm, h * 64, 32, x=xp), share(xp, h * 64 + 32, 32, x=xm))

    def to_pair(d, h):
        return share(d, h * 64, 64, c=other)

    ring = ring_sum("p", project, p1, p1_rx, ra1_p, ra1_m, rb1_p, rb1_m)
    next(ring)
    next(ring)
    next(ring)
    phase("w_out_far")
    arrived(u1c, d1c)
    u2_o, d2_o = up_out(step(y, 2)), dn_out(step(z, 2))
    next(ring)
    next(ring)
    phase("w_on_own")
    arrived(u2_own, d2_own)
    u3_own, d3_own = up_on(y), dn_on(z)
    next(ring)
    norm_chunk(0)
    pair_own0 = to_pair(x, 0)
    first0 = first_out(0)
    rest0 = rest_out(0)
    phase("w_on_minus")
    arrived(u2_m, d2_m)
    u3_m, d3_m = up_on(ym), dn_on(zm)
    next(ring)
    norm_chunk(1)
    pair_own1 = to_pair(x, 1)
    first1 = first_out(1)
    phase("w_on_plus")
    arrived(u2_p, d2_p)
    u3_p, d3_p = up_on(yp), dn_on(zp)
    phase("g0_wait_first")
    arrived(first0)
    on0 = pass_on(0)
    rest1 = rest_out(1)
    phase("w_on_far_u")
    arrived(u2_o)
    u3_o = up_on(step(y, 2))
    phase("g0_wait_rest")
    arrived(rest0)
    pair_near0 = (to_pair(xm, 0), to_pair(xp, 0))
    phase("w_on_far_d")
    arrived(d2_o)
    d3_o = dn_on(step(z, 2))
    phase("g1_wait_first")
    arrived(first1)
    on1 = pass_on(1)
    phase("g0_wait_on")
    arrived(on0)
    pair_far0 = to_pair(xo, 0)
    phase("g1_wait_rest")
    arrived(rest1)
    pair_near1 = (to_pair(xm, 1), to_pair(xp, 1))
    phase("w_wait")
    arrived(u3_own, u3_m, u3_p, d3_own, d3_m, d3_p, u3_o, d3_o)
    phase("g0_wait_pair")
    arrived(pair_near0, (pair_own0, pair_far0))

    ring = ring_sum("m", mix, p2, p2_rx, ra2_p, ra2_m, rb2_p, rb2_m)
    next(ring)
    phase("g1_wait_on")
    arrived(on1)
    pair_far1 = to_pair(xo, 1)
    next(ring)
    phase("g1_wait_pair")
    arrived(pair_near1, (pair_own1, pair_far1))
    for unused in range(4):
        next(ring)

    stores = []
    for h in range(2):
        if h == 1:
            next(ring)
        phase(f"f{h}_final")
        for first in range(0, 64, 32):
            rows = slice(h * 64 + first, h * 64 + first + 32)
            for half in range(2):
                cols = slice(half * 1024, (half + 1) * 1024)
                value = total_of(p2, p2_rx, rb2_p, rb2_m, h, half, first, 32)
                out_s[rows, cols] = (updated[rows, cols].astype(F32) + value).astype(BF16)
        stores.append(fetch(out_s.at[chunk(h), :], out.at[chunk(h), :]))
    phase("s35_finish")
    for copy in stores:
        copy.wait()
    net.finish()
    phase(None)


def body(resid, q, k, v, g, log_decay, wo, gain, up, dn):
    vm = pltpu.VMEM
    scratch = [
        vm((ROWS, DK), BF16), vm((ROWS, DK), BF16), vm((ROWS, DV), BF16), vm((ROWS, DV), BF16),
        vm((DV, D), BF16), vm((128, D), BF16), vm((1, D), F32), vm((BLOCKS, 128), F32),
        vm((4, 128, 128), F32),
        vm((ROWS, 128), F32), vm((BLOCKS, 128), F32), vm((BLOCKS, 128), F32),
        vm((DK, DV), F32), vm((BLOCKS, DK, DV), BF16), vm((ROWS, DV), F32), vm((ROWS, DK), BF16),
        vm((128, DV), BF16), vm((ROWS, DV), F32),
        vm((4, QUARTER, DV), BF16), vm((4, QUARTER, DV), BF16),
        vm((4, QUARTER, DV), BF16), vm((4, QUARTER, DV), BF16),
        vm((QUARTER, DV), BF16), vm((4, QUARTER, DV), BF16),
        vm((8, 128), F32), vm((4, 8, 128), F32), vm((8, 128), F32), vm((4, 8, 128), F32),
        vm((4, 2, 2, 128, 1024), BF16), vm((4, 2, 128, 1024), BF16),
        vm((2, 64, 1024), BF16), vm((2, 64, 1024), BF16),
        vm((2, 2, 64, 1024), BF16), vm((2, 2, 64, 1024), BF16),
        vm((128, D), BF16), vm((4, 2, 128, D), BF16), vm((128, FFL), BF16),
        vm((D, FFL), BF16), vm((FFL, D), BF16),
        vm((4, 2, 2, 128, 1024), BF16), vm((4, 2, 128, 1024), BF16),
        vm((2, 64, 1024), BF16), vm((2, 64, 1024), BF16),
        vm((2, 2, 64, 1024), BF16), vm((2, 2, 64, 1024), BF16),
        vm((128, D), BF16),
        pltpu.SemaphoreType.DMA((N_COPIES,)),
        pltpu.SemaphoreType.DMA((N_COPIES,)),
        pltpu.SemaphoreType.DMA((N_LOCAL,)),
    ]
    anywhere = pl.BlockSpec(memory_space=pl.ANY)
    return pl.pallas_call(
        kernel,
        out_shape=jax.ShapeDtypeStruct((128, D), BF16),
        in_specs=[anywhere] * 11,
        out_specs=anywhere,
        scratch_shapes=scratch,
        compiler_params=pltpu.CompilerParams(
            collective_id=0, has_side_effects=True, vmem_limit_bytes=66_000_000
        ),
    )(
        resid, q, k, v, g, log_decay.reshape(BLOCKS, BLOCK), wo,
        gain.astype(F32).reshape(1, D), up, dn, jnp.asarray(rotation_tables()),
    )


def solution(mesh):
    torus = Mesh(mesh.devices.reshape(4, 4, 4, 2), ("z", "y", "x", "c"))
    sp, tp = ("z", "y"), ("x", "c")
    placed = (
        P(("z", "y", "x", "c"), None),
        P(sp, tp),
        P(sp, tp),
        P(sp, tp),
        P(sp, tp),
        P(tp, sp),
        P(tp, None),
        P(),
        P(sp, tp),
        P(tp, sp),
    )
    return jax.shard_map(
        body, mesh=torus, in_specs=placed, out_specs=P(("z", "y", "x", "c"), None), check_vma=False
    )
```

```python
import jax
import jax.numpy as jnp
import numpy as np
from jax import lax
from jax.experimental import pallas as pl
from jax.experimental.pallas import tpu as pltpu
from jax.sharding import Mesh
from jax.sharding import PartitionSpec as P

DK = 256
DV = 512
HALF = DK // 2
BLOCK = 128
BLOCKS = 8
ROWS = 1024
D = 2048
FFL = 1024
QUARTER = DK // 4
EPS = 1e-06
F32 = jnp.float32
BF16 = jnp.bfloat16


def rotation_tables():
    inverse = 10000.0 ** (-np.arange(0, DK, 2, dtype=np.float64) / DK)
    inside = np.arange(BLOCK, dtype=np.float64)[:, None] * inverse[None, :]
    start = (np.arange(128, dtype=np.float64) * BLOCK)[:, None] * inverse[None, :]
    return np.stack([np.cos(inside), np.sin(inside), np.cos(start), np.sin(start)]).astype(np.float32)


class Phases:
    def __init__(self):
        self.scope = None

    def __call__(self, name):
        if self.scope is not None:
            self.scope.__exit__(None, None, None)
        self.scope = None
        if name is not None:
            self.scope = jax.named_scope(name)
            self.scope.__enter__()


class Copies:
    def __init__(self, send, recv, local, sized):
        self.send, self.recv, self.local, self.sized = send, recv, local, sized
        self.count = self.local_count = 0
        self.sent = {}

    def group(self):
        self.count += 1
        return Group(self, self.recv.at[self.count - 1])

    def start(self, kind, group, src, dst, **where):
        at, size = self.sent.get(kind, (len(self.sent), 0))
        self.sent[kind] = (at, size + bytes_of(src))
        group.size += bytes_of(dst)
        pltpu.make_async_remote_copy(
            src_ref=src,
            dst_ref=dst,
            send_sem=self.send.at[at],
            recv_sem=group.sem,
            device_id=where,
            device_id_type=pl.DeviceIdType.MESH,
        ).start()

    def local_copies(self, *pairs):
        self.local_count += 1
        group = Group(self, self.local.at[self.local_count - 1])
        for src, dst in pairs:
            pltpu.make_async_copy(src, dst, group.sem).start()
            group.size += bytes_of(dst)
        return group

    def finish(self):
        for at, size in self.sent.values():
            view = self.sized(size)
            pltpu.make_async_copy(view, view, self.send.at[at]).wait()


class Group:
    def __init__(self, net, sem):
        self.net, self.sem, self.size = net, sem, 0

    def wait(self):
        view = self.net.sized(self.size)
        pltpu.make_async_copy(view, view, self.sem).wait()


def bytes_of(ref):
    return int(np.prod(ref.shape)) * jnp.dtype(ref.dtype).itemsize


N_SEND = 7
N_RECV = 56
N_LOCAL = 8


def kernel(
    resid, q_in, k_in, v_in, g_in, ld_in, wo_in, gain_in, up_in, dn_in, tab_in, out,
    q_s, k_s, v_s, g_s, wo_s, resid_s, gain_s, ld_s, tab_s,
    ccol, crow, bstart, s_run, s_blk, local, q_late, gated, gate_f,
    st_tx, st_rx, in_tx, in_rx, row_tx, row_rx, dec_tx, dec_rx, rdec_tx, rdec_rx,
    p1, p1_rx, ra1, rb1,
    updated, normed, hidden, up_w, dn_w,
    p2, p2_rx, ra2, rb2, p3, p3_rx, ra3, rb3, out_s,
    send, recv, loc,
):
    z, y = lax.axis_index("z"), lax.axis_index("y")
    x, c = lax.axis_index("x"), lax.axis_index("c")

    def step(a, by):
        return lax.rem(a + by, 4)

    xp, xm, xo = step(x, 1), step(x, 3), step(x, 2)
    yp, ym = step(y, 1), step(y, 3)
    zp, zm = step(z, 1), step(z, 3)
    other = 1 - c
    def sized(size):
        if size % 32768 == 0:
            return up_w.at[0 : size // 2048, :]
        return tab_s.at[0, 0 : size // 512, :]

    net = Copies(send, recv, loc, sized)
    phase = Phases()
    phase("s00_barrier")

    own_rows = pl.ds(pl.multiple_of((4 * z + y) * 128, 128), 128)
    own_cols = pl.ds(pl.multiple_of((4 * y + z) * 128, 128), 128)

    barrier = pltpu.get_barrier_semaphore()
    for where in (
        {"y": yp}, {"y": ym}, {"y": step(y, 2)},
        {"z": zp}, {"z": zm}, {"z": step(z, 2)},
        {"x": xp}, {"x": xm}, {"c": other},
    ):
        pl.semaphore_signal(barrier, inc=1, device_id=where, device_id_type=pl.DeviceIdType.MESH)

    f_ld = net.local_copies((ld_in, ld_s))
    f_kv = net.local_copies((tab_in, tab_s), (k_in, k_s), (v_in, v_s))
    f_qg = net.local_copies((q_in, q_s), (g_in, g_s))
    f_wo = net.local_copies((wo_in, wo_s), (resid, resid_s))
    f_gain = net.local_copies((gain_in, gain_s))
    f_up = net.local_copies((up_in, up_w.at[own_rows, :]))
    f_dn = net.local_copies((dn_in, dn_w.at[:, own_cols]))

    phase("s01_decays")
    f_ld.wait()
    ii = lax.broadcasted_iota(jnp.int32, (BLOCK, BLOCK), 0)
    jj = lax.broadcasted_iota(jnp.int32, (BLOCK, BLOCK), 1)
    causal = ii >= jj
    lower = jnp.where(causal, 1.0, 0.0).astype(F32)
    ld = ld_s[...]
    nt = (((1,), (1,)), ((), ()))
    by_col = lax.dot_general(lower, ld, nt, precision=lax.Precision.HIGHEST, preferred_element_type=F32)
    crow[...] = lax.dot_general(ld, lower, nt, precision=lax.Precision.HIGHEST, preferred_element_type=F32)
    for n in range(BLOCKS):
        ccol[n * BLOCK : (n + 1) * BLOCK, :] = jnp.broadcast_to(by_col[:, n : n + 1], (BLOCK, 128))

    phase("s02_kvwait")
    whole = sum(ccol[n * BLOCK + BLOCK - 1 : (n + 1) * BLOCK, :] for n in range(BLOCKS))
    dec_tx[...] = jnp.broadcast_to(whole, (8, 128))
    dec_rx[y] = jnp.broadcast_to(whole, (8, 128))

    f_kv.wait()

    def rotated(ref, n):
        rows = pl.ds(pl.multiple_of(n * BLOCK, BLOCK), BLOCK)
        block = (4 * z + y) * BLOCKS + n
        cos_in, sin_in = tab_s[0], tab_s[1]
        cos_at = tab_s[2, pl.ds(block, 1), :]
        sin_at = tab_s[3, pl.ds(block, 1), :]
        cosine = cos_at * cos_in - sin_at * sin_in
        sine = sin_at * cos_in + cos_at * sin_in
        first = ref[rows, 0:HALF].astype(F32)
        second = ref[rows, HALF:DK].astype(F32)
        return rows, first * cosine - second * sine, first * sine + second * cosine

    phase("s03_states")
    s_run[...] = jnp.zeros_like(s_run)

    def state_block(n, before):
        rows, a, b = rotated(k_s, n)
        a = (a * DK**-0.5).astype(BF16)
        b = (b * DK**-0.5).astype(BF16)
        k_s[rows, 0:HALF] = a
        k_s[rows, HALF:DK] = b
        total = ccol[pl.ds(n * BLOCK + BLOCK - 1, 1), :]
        to_end = jnp.exp(total - ccol[rows, :])
        decayed = jnp.concatenate(
            [(a.astype(F32) * to_end).astype(BF16), (b.astype(F32) * to_end).astype(BF16)], axis=1
        )
        term = lax.dot_general(
            decayed, v_s[rows, :], (((0,), (0,)), ((), ())), preferred_element_type=F32
        )
        s_blk[n] = s_run[...].astype(BF16)
        s_run[...] = jnp.exp(total[:, 0:1]) * s_run[...] + term
        bstart[pl.ds(n, 1), :] = before
        return before + total

    total = lax.fori_loop(0, 4, state_block, jnp.zeros((1, 128), F32), unroll=True)
    phase("s03b_barrier")
    pl.semaphore_wait(barrier, 9)
    dec_copies = net.group()
    for by in (2, 1, 3):
        net.start("decay", dec_copies, dec_tx, dec_rx.at[y], y=step(y, by))

    def up_at(zz, yy, half=None):
        first, size = (0, 128) if half is None else (half * 64, 64)
        return up_w.at[pl.ds(pl.multiple_of(zz * 512 + yy * 128 + first, 64), size), :]

    def dn_at(yy, zz, half=None):
        cols = pl.ds(pl.multiple_of(yy * 512 + zz * 128, 128), 128)
        return dn_w.at[:, cols] if half is None else dn_w.at[half * 512 : half * 512 + 512, cols]

    def up_own(half):
        return up_in.at[half * 64 : half * 64 + 64, :]

    def dn_own(half):
        return dn_in.at[half * 512 : half * 512 + 512, :]

    def two(kind, axis, plus, minus, group=None):
        group = net.group() if group is None else group
        ahead, behind = {"x": (xp, xm), "y": (yp, ym), "z": (zp, zm)}[axis]
        for to, (src, dst) in ((ahead, plus), (behind, minus)):
            net.start(kind, group, src, dst, **{axis: to})
        return group

    d1a = two("down", "z", (dn_own(0), dn_at(y, z, 0)), (dn_own(1), dn_at(y, z, 1)))
    d1b = two("down", "z", (dn_own(1), dn_at(y, z, 1)), (dn_own(0), dn_at(y, z, 0)))
    phase("s03c_states")
    lax.fori_loop(4, BLOCKS, state_block, total, unroll=True)

    phase("s04_sendstate")
    for part in range(4):
        st_tx[part] = s_run[part * QUARTER : (part + 1) * QUARTER, :].astype(BF16)
    st_copies = net.group()
    for by in (2, 1, 3):
        to = step(y, by)
        net.start("state", st_copies, st_tx.at[to], st_rx.at[y], y=to)
    st_rx[y] = st_tx[y]

    def arrived(*groups):
        for group in groups:
            group.wait()

    def twice(ref):
        return ref, ref

    def up_out(yy):
        return two("up", "z", twice(up_at(z, yy)), twice(up_at(z, yy)))

    def dn_out(zz):
        return two("down", "y", twice(dn_at(y, zz)), twice(dn_at(y, zz)))

    def up_on(*ys):
        for yy in ys:
            two("up", "z", twice(up_at(zm, yy, 0)), twice(up_at(zp, yy, 1)), up_last)

    def dn_on(*zs):
        for zz in zs:
            two("down", "y", twice(dn_at(ym, zz, 0)), twice(dn_at(yp, zz, 1)), dn_last)

    up_last, dn_last = net.group(), net.group()

    phase("s06_local1")
    f_qg.wait()

    def local_block(n, carry):
        rows, a, b = rotated(q_s, n)
        col = ccol[rows, :]
        a = a.astype(BF16)
        b = b.astype(BF16)
        query = jnp.concatenate([a, b], axis=1)
        scores = lax.dot_general(query, k_s[rows, :], nt, preferred_element_type=F32)
        spread = col - crow[pl.ds(n, 1), :]
        factor = jnp.where(causal, jnp.exp(jnp.minimum(spread, 0.0)), 0.0)
        weights = (scores * factor).astype(BF16)
        a = a.astype(F32)
        b = b.astype(F32)
        early = jnp.exp(col)
        decayed = jnp.concatenate([(a * early).astype(BF16), (b * early).astype(BF16)], axis=1)
        late = jnp.exp(col + bstart[pl.ds(n, 1), :])
        q_late[rows, 0:HALF] = (a * late).astype(BF16)
        q_late[rows, HALF:DK] = (b * late).astype(BF16)
        local[rows, :] = jnp.dot(
            weights, v_s[rows, :], preferred_element_type=F32
        ) + jnp.dot(decayed, s_blk[n], preferred_element_type=F32)
        return carry

    lax.fori_loop(0, 4, local_block, 0)

    dec_copies.wait()
    log_row = dec_rx[0] + dec_rx[1] + dec_rx[2] + dec_rx[3]
    rdec_tx[...] = log_row
    rdec_rx[z] = log_row
    rdec_copies = net.group()
    for by in (2, 1, 3):
        net.start("decay", rdec_copies, rdec_tx, rdec_rx.at[z], z=step(z, by))

    def gate_block(n, carry):
        rows = pl.ds(pl.multiple_of(n * 64, 64), 64)
        gate = g_s[rows, :].astype(F32)
        gate_f[rows, :] = gate / (1.0 + jnp.exp(-gate))
        return carry

    lax.fori_loop(0, 16, gate_block, 0)
    u1a = two("up", "y", (up_own(0), up_at(z, y, 0)), (up_own(1), up_at(z, y, 1)))

    phase("s07_waitstate")
    st_copies.wait()
    phase("s08_rowtotal")
    run = st_rx[0].astype(F32)
    for at in range(1, 4):
        run = jnp.exp(dec_rx[at][0:1, 0:1]) * run + st_rx[at].astype(F32)
    row_tx[...] = run.astype(BF16)
    row_rx[z] = run.astype(BF16)
    row_copies = net.group()
    for by in (2, 1, 3):
        net.start("state", row_copies, row_tx, row_rx.at[z], z=step(z, by))

    u1b = two("up", "y", (up_own(1), up_at(z, y, 1)), (up_own(0), up_at(z, y, 0)))
    phase("s09b_w")
    arrived(d1a)
    d1c = two("down", "z", twice(dn_at(y, zm, 0)), twice(dn_at(y, zp, 1)))
    f_up.wait()
    u2_own = up_out(y)
    phase("s09_local2")
    lax.fori_loop(4, 8, local_block, 0)
    phase("s10_waitrow")

    rdec_copies.wait()
    row_copies.wait()
    phase("s11_incoming")
    run = jnp.zeros((QUARTER, DV), F32)
    for at in range(4):
        later = jnp.exp(rdec_rx[at][0:1, 0:1]) * run + row_rx[at].astype(F32)
        run = jnp.where(at < z, later, run)
    for at in range(4):
        in_tx[at] = run.astype(BF16)
        if at < 3:
            run = jnp.exp(dec_rx[at][0:1, 0:1]) * run + st_rx[at].astype(F32)
    in_copies = net.group()
    for by in (2, 1, 3):
        to = step(y, by)
        net.start("state", in_copies, in_tx.at[to], in_rx.at[y], y=to)
    in_rx[y] = in_tx[y]

    phase("s13_waitin")
    f_wo.wait()
    f_gain.wait()
    in_copies.wait()
    phase("s12_w2wait")
    arrived(u1a)
    u1c = two("up", "y", twice(up_at(z, ym, 0)), twice(up_at(z, yp, 1)))
    f_dn.wait()
    d2_own = dn_out(z)
    arrived(u1b, d1b)
    u2_m, u2_p = up_out(ym), up_out(yp)
    d2_m, d2_p = dn_out(zm), dn_out(zp)
    def chunk(h):
        return slice(h * 64, h * 64 + 64)

    def project(d, h):
        picks = [pl.ds(pl.multiple_of(d * 256 + i * 128 + h * 64, 64), 64) for i in range(2)]

        def both(ref):
            return jnp.concatenate([ref[rows, :] for rows in picks], axis=0)

        incoming = jnp.concatenate([in_rx[at] for at in range(4)], axis=0)
        kept = both(local) + jnp.dot(both(q_late), incoming, preferred_element_type=F32)
        scale = lax.rsqrt(jnp.mean(kept * kept, axis=-1, keepdims=True) + EPS)
        gated[...] = (both(gate_f) * kept * scale).astype(BF16)
        for j in range(4):
            part = jnp.dot(
                gated[...], wo_s[:, j * 512 : (j + 1) * 512], preferred_element_type=F32
            ).astype(BF16)
            to = slice((j % 2) * 512, (j % 2) * 512 + 512)
            p1[h, d, 0, j // 2, :, to] = part[0:64]
            p1[h, d, 1, j // 2, :, to] = part[64:128]

    def mix_up(d, h):
        rows = normed[d, :, chunk(h), :].reshape(128, D)
        for j in range(2):
            cols = slice(j * 512, (j + 1) * 512)
            pre = jnp.maximum(jnp.dot(rows, up_w[:, cols], preferred_element_type=F32), 0.0)
            hidden[d, h, :, cols] = (pre * pre).astype(BF16)

    order = (y, ym, yp, step(y, 2))

    def dn_cols(k):
        return dn_w[:, pl.ds(pl.multiple_of(order[k] * 512, 512), 512)]

    def mix_down(d, h):
        for k in range(3):
            part = jnp.dot(hidden[d, h], dn_cols(k), preferred_element_type=F32).astype(BF16)
            for core in range(2):
                rows = slice(core * 64, core * 64 + 64)
                for at in range(0, 512, 256):
                    col = k * 512 + at
                    p2[h, d, core, col // 768, :, col % 768 : col % 768 + 256] = part[rows, at : at + 256]

    def mix_last(d, unused):
        part = jnp.dot(
            hidden[d].reshape(256, FFL), dn_cols(3), preferred_element_type=F32
        ).astype(BF16)
        for h in range(2):
            for core in range(2):
                at = h * 128 + core * 64
                for half in range(2):
                    p3[d, core, half, chunk(h), :] = part[at : at + 64, half * 256 : half * 256 + 256]

    class RingSum:
        blocks = {"xo": xo, "xp": xp, "xm": xm, "x": x}

        def __init__(self, name, compute, arg, p, p_rx, ra, rb):
            self.name, self.compute, self.arg = name, compute, arg
            self.p, self.p_rx = p, p_rx
            self.ra_p, self.ra_m, self.rb_p, self.rb_m = ra.at[0], ra.at[1], rb.at[0], rb.at[1]
            self.pairs, self.a, self.done = {}, net.group(), net.group()
            self.kind = name[0]

        def add(self, d, half, extra):
            total = self.p[d, c, half].astype(F32) + extra.astype(F32)
            self.p[d, c, half] = total.astype(BF16)

        def work(self, *keys):
            for key in keys:
                phase(f"{self.name}_work_{key}")
                d = self.blocks[key]
                self.compute(d, self.arg)
                self.pairs[key] = self.done if key == "x" else net.group()
                net.start(self.kind, self.pairs[key], self.p.at[d, other], self.p_rx.at[d], c=other)

        def pair_sum(self, key):
            phase(f"{self.name}_pair_{key}")
            d = self.blocks[key]
            self.pairs[key].wait()
            for half in range(2):
                self.add(d, half, self.p_rx[d, half])

        def piece(self, d, half):
            return self.p.at[d, c, half]

        def send(self, group, src, dst, to):
            net.start(self.kind, group, src, dst, x=to)

        def send_a(self):
            self.pair_sum("xo")
            self.send(self.a, self.piece(xo, 0), self.ra_p, xp)
            self.send(self.a, self.piece(xo, 1), self.ra_m, xm)

        def send_b(self):
            self.pair_sum("xp")
            self.send(self.done, self.piece(xp, 1), self.rb_p.at[1], xp)
            self.pair_sum("xm")
            self.send(self.done, self.piece(xm, 0), self.rb_m.at[0], xm)

        def send_c(self):
            phase(f"{self.name}_wait_a")
            self.a.wait()
            self.add(xp, 0, self.ra_p[...])
            self.send(self.done, self.piece(xp, 0), self.rb_p.at[0], xp)
            self.add(xm, 1, self.ra_m[...])
            self.send(self.done, self.piece(xm, 1), self.rb_m.at[1], xm)

        def complete(self):
            phase(f"{self.name}_wait_bc")
            self.done.wait()

        def total(self, half, rows, cols):
            value = self.p[x, c, half, rows, cols].astype(F32) + self.p_rx[x, half, rows, cols].astype(F32)
            sides = self.rb_p[half, rows, cols].astype(F32) + self.rb_m[half, rows, cols].astype(F32)
            return value + sides

    rings1 = [RingSum(f"p{h}", project, h, p1.at[h], p1_rx.at[h], ra1.at[h], rb1.at[h]) for h in range(2)]

    def norm_chunk(h):
        phase(f"n{h}_norm")
        gain = gain_s[...].astype(F32).reshape(1, D)
        for first in range(0, 64, 32):
            rows = slice(h * 64 + first, h * 64 + first + 32)
            halves = []
            for half in range(2):
                cols = slice(half * 1024, (half + 1) * 1024)
                value = rings1[h].total(half, slice(first, first + 32), slice(None))
                value = (resid_s[rows, cols].astype(F32) + value).astype(BF16)
                updated[rows, cols] = value
                halves.append(value.astype(F32))
            square = sum(jnp.sum(v * v, axis=-1, keepdims=True) for v in halves)
            scale = lax.rsqrt(square * (1.0 / D) + EPS)
            for half in range(2):
                cols = slice(half * 1024, (half + 1) * 1024)
                normed[x, c, rows, cols] = (halves[half] * scale * gain[:, cols]).astype(BF16)

    def rows_at(d, first, size):
        return twice(normed.at[d, c, first : first + size, :])

    def first_out(h):
        return two("gather", "x", rows_at(x, h * 64, 32), rows_at(x, h * 64 + 32, 32))

    def rest_out(h):
        return two("gather", "x", rows_at(x, h * 64 + 32, 32), rows_at(x, h * 64, 32))

    def pass_on(h):
        return two("gather", "x", rows_at(xm, h * 64, 32), rows_at(xp, h * 64 + 32, 32))

    def to_pair(d, h, group):
        net.start("gather", group, *rows_at(d, h * 64, 64), c=other)

    near = [net.group() for h in range(2)]
    far = [net.group() for h in range(2)]

    r0, r1 = rings1
    r0.work("xo", "xp")
    r0.send_a()
    r0.work("xm")
    r1.work("xo")
    r0.send_b()
    r1.work("xp")
    r1.send_a()
    r1.work("xm", "x")
    r0.work("x")
    phase("w_out_far")
    arrived(u1c, d1c)
    u2_o, d2_o = up_out(step(y, 2)), dn_out(step(z, 2))
    r0.send_c()
    r1.send_b()
    r1.send_c()
    phase("w_on_own")
    arrived(u2_own, d2_own)
    up_on(y)
    dn_on(z)
    r0.complete()
    norm_chunk(0)
    to_pair(x, 0, near[0])
    first0 = first_out(0)
    rest0 = rest_out(0)
    phase("w_on_minus")
    arrived(u2_m, d2_m)
    up_on(ym)
    dn_on(zm)
    r1.complete()
    norm_chunk(1)
    to_pair(x, 1, near[1])
    first1 = first_out(1)
    rest1 = rest_out(1)
    phase("w_on_plus")
    arrived(u2_p, d2_p)
    up_on(yp)
    dn_on(zp)
    phase("g0_wait_first")
    arrived(first0)
    on0 = pass_on(0)
    phase("w_on_far_u")
    arrived(u2_o)
    up_on(step(y, 2))
    phase("g0_wait_rest")
    arrived(rest0)
    for d in (xm, xp):
        to_pair(d, 0, near[0])
    phase("w_on_far_d")
    arrived(d2_o)
    dn_on(step(z, 2))
    phase("g1_wait_first")
    arrived(first1)
    on1 = pass_on(1)
    phase("g0_wait_pair")
    arrived(near[0])
    phase("w_wait_up")
    arrived(up_last)

    r0, r1 = [
        RingSum(f"m{h}", mix_down, h, p2.at[h], p2_rx.at[h], ra2.at[h], rb2.at[h]) for h in range(2)
    ]
    r2 = RingSum("m2", mix_last, None, p3, p3_rx, ra3, rb3)
    phase("m0_up_near")
    mix_up(xp, 0)
    mix_up(xm, 0)
    phase("g1_wait_rest")
    arrived(rest1)
    for d in (xm, xp):
        to_pair(d, 1, near[1])
    r0.work("xp", "xm")
    phase("g0_wait_on")
    arrived(on0)
    to_pair(xo, 0, far[0])
    phase("g1_wait_pair")
    arrived(near[1])
    phase("m1_up_near")
    mix_up(xp, 1)
    mix_up(xm, 1)
    r0.send_b()
    r1.work("xp", "xm")
    phase("g0_wait_far")
    arrived(far[0])
    phase("m0_up_far")
    mix_up(xo, 0)
    r0.work("xo")
    r1.send_b()
    phase("g1_wait_on")
    arrived(on1)
    to_pair(xo, 1, far[1])
    phase("m0_up_own")
    mix_up(x, 0)
    r0.send_a()
    phase("m1_up_own")
    mix_up(x, 1)
    phase("g1_wait_far")
    arrived(far[1])
    phase("m1_up_far")
    mix_up(xo, 1)
    r1.work("xo")
    phase("w_wait_last")
    arrived(dn_last)
    r2.work("xo")
    r1.send_a()
    r2.work("xp")
    r2.send_a()
    r0.send_c()
    r2.work("xm")
    r1.send_c()
    r2.send_b()
    r0.work("x")
    r1.work("x")
    r2.work("x")
    r2.send_c()

    def finish_columns(k, rows, total_at):
        for zz in range(4):
            cols = pl.ds(pl.multiple_of((4 * zz + order[k]) * 128, 128), 128)
            out_s[rows, cols] = (updated[rows, cols].astype(F32) + total_at(zz * 128)).astype(BF16)

    def chunk_total(ring, k):
        def at(first):
            col = k * 512 + first
            return ring.total(col // 768, slice(None), slice(col % 768, col % 768 + 128))

        return at

    for h, ring in enumerate((r0, r1)):
        ring.complete()
        phase(f"f{h}_final")
        for k in range(3):
            finish_columns(k, chunk(h), chunk_total(ring, k))
    r2.complete()
    phase("f2_final")
    finish_columns(3, slice(None), lambda first: r2.total(first // 256, slice(None), slice(first % 256, first % 256 + 128)))
    store = net.local_copies((out_s, out))
    phase("s35_finish")
    store.wait()
    net.finish()
    phase(None)


def body(resid, q, k, v, g, log_decay, wo, gain, up, dn):
    vm = pltpu.VMEM
    scratch = [
        vm((ROWS, DK), BF16), vm((ROWS, DK), BF16), vm((ROWS, DV), BF16), vm((ROWS, DV), BF16),
        vm((DV, D), BF16), vm((128, D), BF16), vm((D,), BF16), vm((BLOCKS, 128), F32),
        vm((4, 128, 128), F32),
        vm((ROWS, 128), F32), vm((BLOCKS, 128), F32), vm((BLOCKS, 128), F32),
        vm((DK, DV), F32), vm((BLOCKS, DK, DV), BF16), vm((ROWS, DV), F32), vm((ROWS, DK), BF16),
        vm((128, DV), BF16), vm((ROWS, DV), F32),
        vm((4, QUARTER, DV), BF16), vm((4, QUARTER, DV), BF16),
        vm((4, QUARTER, DV), BF16), vm((4, QUARTER, DV), BF16),
        vm((QUARTER, DV), BF16), vm((4, QUARTER, DV), BF16),
        vm((8, 128), F32), vm((4, 8, 128), F32), vm((8, 128), F32), vm((4, 8, 128), F32),
        vm((2, 4, 2, 2, 64, 1024), BF16), vm((2, 4, 2, 64, 1024), BF16),
        vm((2, 2, 64, 1024), BF16), vm((2, 2, 2, 64, 1024), BF16),
        vm((128, D), BF16), vm((4, 2, 128, D), BF16), vm((4, 2, 128, FFL), BF16),
        vm((D, FFL), BF16), vm((FFL, D), BF16),
        vm((2, 4, 2, 2, 64, 768), BF16), vm((2, 4, 2, 64, 768), BF16),
        vm((2, 2, 64, 768), BF16), vm((2, 2, 2, 64, 768), BF16),
        vm((4, 2, 2, 128, 256), BF16), vm((4, 2, 128, 256), BF16),
        vm((2, 128, 256), BF16), vm((2, 2, 128, 256), BF16),
        vm((128, D), BF16),
        pltpu.SemaphoreType.DMA((N_SEND,)),
        pltpu.SemaphoreType.DMA((N_RECV,)),
        pltpu.SemaphoreType.DMA((N_LOCAL,)),
    ]
    anywhere = pl.BlockSpec(memory_space=pl.ANY)
    return pl.pallas_call(
        kernel,
        out_shape=jax.ShapeDtypeStruct((128, D), BF16),
        in_specs=[anywhere] * 11,
        out_specs=anywhere,
        scratch_shapes=scratch,
        compiler_params=pltpu.CompilerParams(
            collective_id=0, has_side_effects=True, vmem_limit_bytes=66_000_000
        ),
    )(
        resid, q, k, v, g, log_decay.reshape(BLOCKS, BLOCK), wo,
        gain, up, dn, jnp.asarray(rotation_tables()),
    )


def solution(mesh):
    torus = Mesh(mesh.devices.reshape(4, 4, 4, 2), ("z", "y", "x", "c"))
    sp, tp = ("z", "y"), ("x", "c")
    placed = (
        P(("z", "y", "x", "c"), None),
        P(sp, tp),
        P(sp, tp),
        P(sp, tp),
        P(sp, tp),
        P(tp, sp),
        P(tp, None),
        P(),
        P(sp, tp),
        P(tp, sp),
    )
    return jax.shard_map(
        body, mesh=torus, in_specs=placed, out_specs=P(("z", "y", "x", "c"), None), check_vma=False
    )
```

```python
import jax
import jax.numpy as jnp
import numpy as np
from jax import lax
from jax.experimental import pallas as pl
from jax.experimental.pallas import tpu as pltpu
from jax.sharding import Mesh
from jax.sharding import PartitionSpec as P

DK = 256
DV = 512
HALF = DK // 2
BLOCK = 128
BLOCKS = 8
ROWS = 1024
D = 2048
FFL = 1024
QUARTER = DK // 4
EPS = 1e-06
F32 = jnp.float32
BF16 = jnp.bfloat16


def rotation_tables():
    inverse = 10000.0 ** (-np.arange(0, DK, 2, dtype=np.float64) / DK)
    inside = np.arange(BLOCK, dtype=np.float64)[:, None] * inverse[None, :]
    start = (np.arange(128, dtype=np.float64) * BLOCK)[:, None] * inverse[None, :]
    return np.stack([np.cos(inside), np.sin(inside), np.cos(start), np.sin(start)]).astype(np.float32)


class Phases:
    def __init__(self):
        self.scope = None

    def __call__(self, name):
        if self.scope is not None:
            self.scope.__exit__(None, None, None)
        self.scope = None
        if name is not None:
            self.scope = jax.named_scope(name)
            self.scope.__enter__()


class Copies:
    def __init__(self, send, recv, local, sized):
        self.send, self.recv, self.local, self.sized = send, recv, local, sized
        self.count = self.local_count = 0
        self.sent = {}

    def group(self):
        self.count += 1
        return Group(self, self.recv.at[self.count - 1])

    def start(self, kind, group, src, dst, **where):
        if kind is None:
            at = N_SEND - 1
        else:
            at, size = self.sent.get(kind, (len(self.sent), 0))
            self.sent[kind] = (at, size + bytes_of(src))
        group.size += bytes_of(dst)
        pltpu.make_async_remote_copy(
            src_ref=src,
            dst_ref=dst,
            send_sem=self.send.at[at],
            recv_sem=group.sem,
            device_id=where,
            device_id_type=pl.DeviceIdType.MESH,
        ).start()

    def local_copies(self, *pairs):
        self.local_count += 1
        group = Group(self, self.local.at[self.local_count - 1])
        for src, dst in pairs:
            pltpu.make_async_copy(src, dst, group.sem).start()
            group.size += bytes_of(dst)
        return group

    def finish(self):
        for at, size in self.sent.values():
            view = self.sized(size)
            pltpu.make_async_copy(view, view, self.send.at[at]).wait()


class Group:
    def __init__(self, net, sem):
        self.net, self.sem, self.size = net, sem, 0

    def wait(self, size=None):
        view = self.net.sized(self.size if size is None else size)
        pltpu.make_async_copy(view, view, self.sem).wait()


def bytes_of(ref):
    return int(np.prod(ref.shape)) * jnp.dtype(ref.dtype).itemsize


N_SEND = 8
N_RECV = 56
N_LOCAL = 8


def kernel(
    resid, q_in, k_in, v_in, g_in, ld_in, wo_in, gain_in, up_in, dn_in, tab_in, out,
    q_s, k_s, v_s, g_s, wo_s, resid_s, gain_s, ld_s, tab_s,
    ccol, crow, bstart, s_run, s_blk, local, q_late, gated, gate_f,
    st_tx, st_rx, in_tx, in_rx, row_tx, row_rx, dec_tx, dec_rx, rdec_tx, rdec_rx,
    p1, p1_rx, ra1, rb1,
    updated, normed, hidden, up_w, dn_w,
    p2, p2_rx, ra2, rb2, p3, p3_rx, ra3, rb3, out_s,
    send, recv, loc,
):
    z, y = lax.axis_index("z"), lax.axis_index("y")
    x, c = lax.axis_index("x"), lax.axis_index("c")

    def step(a, by):
        return lax.rem(a + by, 4)

    xp, xm, xo = step(x, 1), step(x, 3), step(x, 2)
    yp, ym = step(y, 1), step(y, 3)
    zp, zm = step(z, 1), step(z, 3)
    other = 1 - c
    def sized(size):
        if size % 32768 == 0:
            return up_w.at[0 : size // 2048, :]
        return tab_s.at[0, 0 : size // 512, :]

    net = Copies(send, recv, loc, sized)
    phase = Phases()
    phase("s00_barrier")

    own_rows = pl.ds(pl.multiple_of((4 * z + y) * 128, 128), 128)
    own_cols = pl.ds(pl.multiple_of((4 * y + z) * 128, 128), 128)

    barrier = pltpu.get_barrier_semaphore()
    for where in (
        {"y": yp}, {"y": ym}, {"y": step(y, 2)},
        {"z": zp}, {"z": zm}, {"z": step(z, 2)},
        {"x": xp}, {"x": xm}, {"c": other},
    ):
        pl.semaphore_signal(barrier, inc=1, device_id=where, device_id_type=pl.DeviceIdType.MESH)

    f_ld = net.local_copies((ld_in, ld_s))
    f_kv = net.local_copies((tab_in, tab_s), (k_in, k_s), (v_in, v_s))
    f_qg = net.local_copies((q_in, q_s), (g_in, g_s))
    f_wo = net.local_copies((wo_in, wo_s), (resid, resid_s))
    f_gain = net.local_copies((gain_in, gain_s))
    f_up = net.local_copies((up_in, up_w.at[own_rows, :]))
    f_dn = net.local_copies((dn_in, dn_w.at[:, own_cols]))

    phase("s01_decays")
    f_ld.wait()
    ii = lax.broadcasted_iota(jnp.int32, (BLOCK, BLOCK), 0)
    jj = lax.broadcasted_iota(jnp.int32, (BLOCK, BLOCK), 1)
    causal = ii >= jj
    lower = jnp.where(causal, 1.0, 0.0).astype(F32)
    ld = ld_s[...]
    nt = (((1,), (1,)), ((), ()))
    by_col = lax.dot_general(lower, ld, nt, precision=lax.Precision.HIGHEST, preferred_element_type=F32)
    crow[...] = lax.dot_general(ld, lower, nt, precision=lax.Precision.HIGHEST, preferred_element_type=F32)
    for n in range(BLOCKS):
        ccol[n * BLOCK : (n + 1) * BLOCK, :] = jnp.broadcast_to(by_col[:, n : n + 1], (BLOCK, 128))

    phase("s02_kvwait")
    whole = sum(ccol[n * BLOCK + BLOCK - 1 : (n + 1) * BLOCK, :] for n in range(BLOCKS))
    dec_tx[...] = jnp.broadcast_to(whole, (8, 128))
    dec_rx[y] = jnp.broadcast_to(whole, (8, 128))

    f_kv.wait()

    def rotated(ref, n):
        rows = pl.ds(pl.multiple_of(n * BLOCK, BLOCK), BLOCK)
        block = (4 * z + y) * BLOCKS + n
        cos_in, sin_in = tab_s[0], tab_s[1]
        cos_at = tab_s[2, pl.ds(block, 1), :]
        sin_at = tab_s[3, pl.ds(block, 1), :]
        cosine = cos_at * cos_in - sin_at * sin_in
        sine = sin_at * cos_in + cos_at * sin_in
        first = ref[rows, 0:HALF].astype(F32)
        second = ref[rows, HALF:DK].astype(F32)
        return rows, first * cosine - second * sine, first * sine + second * cosine

    phase("s03_states")
    s_run[...] = jnp.zeros_like(s_run)

    def state_block(n, before):
        rows, a, b = rotated(k_s, n)
        a = (a * DK**-0.5).astype(BF16)
        b = (b * DK**-0.5).astype(BF16)
        k_s[rows, 0:HALF] = a
        k_s[rows, HALF:DK] = b
        total = ccol[pl.ds(n * BLOCK + BLOCK - 1, 1), :]
        to_end = jnp.exp(total - ccol[rows, :])
        decayed = jnp.concatenate(
            [(a.astype(F32) * to_end).astype(BF16), (b.astype(F32) * to_end).astype(BF16)], axis=1
        )
        term = lax.dot_general(
            decayed, v_s[rows, :], (((0,), (0,)), ((), ())), preferred_element_type=F32
        )
        s_blk[n] = s_run[...].astype(BF16)
        s_run[...] = jnp.exp(total[:, 0:1]) * s_run[...] + term
        bstart[pl.ds(n, 1), :] = before
        return before + total

    total = lax.fori_loop(0, 4, state_block, jnp.zeros((1, 128), F32), unroll=True)
    phase("s03b_barrier")
    pl.semaphore_wait(barrier, 9)
    dec_copies = net.group()
    for by in (2, 1, 3):
        net.start("decay", dec_copies, dec_tx, dec_rx.at[y], y=step(y, by))

    def up_at(zz, yy, half=None):
        first, size = (0, 128) if half is None else (half * 64, 64)
        return up_w.at[pl.ds(pl.multiple_of(zz * 512 + yy * 128 + first, 64), size), :]

    def dn_at(yy, zz, half=None):
        cols = pl.ds(pl.multiple_of(yy * 512 + zz * 128, 128), 128)
        return dn_w.at[:, cols] if half is None else dn_w.at[half * 512 : half * 512 + 512, cols]

    def up_own(half):
        return up_in.at[half * 64 : half * 64 + 64, :]

    def dn_own(half):
        return dn_in.at[half * 512 : half * 512 + 512, :]

    def two(kind, axis, plus, minus, group=None):
        group = net.group() if group is None else group
        ahead, behind = {"x": (xp, xm), "y": (yp, ym), "z": (zp, zm)}[axis]
        for to, (src, dst) in ((ahead, plus), (behind, minus)):
            net.start(kind, group, src, dst, **{axis: to})
        return group

    d1a = two("down", "z", (dn_own(0), dn_at(y, z, 0)), (dn_own(1), dn_at(y, z, 1)))
    d1b = two("down", "z", (dn_own(1), dn_at(y, z, 1)), (dn_own(0), dn_at(y, z, 0)))
    phase("s03c_states")
    lax.fori_loop(4, BLOCKS, state_block, total, unroll=True)

    phase("s04_sendstate")
    for part in range(4):
        st_tx[part] = s_run[part * QUARTER : (part + 1) * QUARTER, :].astype(BF16)
    st_copies = net.group()
    for by in (2, 1, 3):
        to = step(y, by)
        net.start("state", st_copies, st_tx.at[to], st_rx.at[y], y=to)
    st_rx[y] = st_tx[y]

    def arrived(*groups):
        for group in groups:
            group.wait()

    def twice(ref):
        return ref, ref

    def up_out(yy):
        return two("up", "z", twice(up_at(z, yy)), twice(up_at(z, yy)))

    def dn_out(zz):
        return two("down", "y", twice(dn_at(y, zz)), twice(dn_at(y, zz)))

    def up_on(*ys):
        for yy in ys:
            two("up", "z", twice(up_at(zm, yy, 0)), twice(up_at(zp, yy, 1)), up_last)

    def dn_on(*zs):
        for zz in zs:
            two("down", "y", twice(dn_at(ym, zz, 0)), twice(dn_at(yp, zz, 1)), dn_last)

    up_last, dn_last = net.group(), net.group()

    phase("s06_local1")
    f_qg.wait()

    def local_block(n, carry):
        rows, a, b = rotated(q_s, n)
        col = ccol[rows, :]
        a = a.astype(BF16)
        b = b.astype(BF16)
        query = jnp.concatenate([a, b], axis=1)
        scores = lax.dot_general(query, k_s[rows, :], nt, preferred_element_type=F32)
        spread = col - crow[pl.ds(n, 1), :]
        factor = jnp.where(causal, jnp.exp(jnp.minimum(spread, 0.0)), 0.0)
        weights = (scores * factor).astype(BF16)
        a = a.astype(F32)
        b = b.astype(F32)
        early = jnp.exp(col)
        decayed = jnp.concatenate([(a * early).astype(BF16), (b * early).astype(BF16)], axis=1)
        late = jnp.exp(col + bstart[pl.ds(n, 1), :])
        q_late[rows, 0:HALF] = (a * late).astype(BF16)
        q_late[rows, HALF:DK] = (b * late).astype(BF16)
        local[rows, :] = jnp.dot(
            weights, v_s[rows, :], preferred_element_type=F32
        ) + jnp.dot(decayed, s_blk[n], preferred_element_type=F32)
        return carry

    lax.fori_loop(0, 4, local_block, 0)

    dec_copies.wait()
    log_row = dec_rx[0] + dec_rx[1] + dec_rx[2] + dec_rx[3]
    rdec_tx[...] = log_row
    rdec_rx[z] = log_row
    rdec_copies = net.group()
    for by in (2, 1, 3):
        net.start("decay", rdec_copies, rdec_tx, rdec_rx.at[z], z=step(z, by))

    def gate_block(n, carry):
        rows = pl.ds(pl.multiple_of(n * 64, 64), 64)
        gate = g_s[rows, :].astype(F32)
        gate_f[rows, :] = gate / (1.0 + jnp.exp(-gate))
        return carry

    lax.fori_loop(0, 16, gate_block, 0)
    u1a = two("up", "y", (up_own(0), up_at(z, y, 0)), (up_own(1), up_at(z, y, 1)))

    phase("s07_waitstate")
    st_copies.wait()
    phase("s08_rowtotal")
    run = st_rx[0].astype(F32)
    for at in range(1, 4):
        run = jnp.exp(dec_rx[at][0:1, 0:1]) * run + st_rx[at].astype(F32)
    row_tx[...] = run.astype(BF16)
    row_copies = net.group()
    for later in (3, 2, 1):

        @pl.when(z < later)
        def _():
            net.start(None, row_copies, row_tx, row_rx.at[z], z=later)


    u1b = two("up", "y", (up_own(1), up_at(z, y, 1)), (up_own(0), up_at(z, y, 0)))
    phase("s09b_w")
    arrived(d1a)
    d1c = two("down", "z", twice(dn_at(y, zm, 0)), twice(dn_at(y, zp, 1)))
    f_up.wait()
    u2_own = up_out(y)
    phase("s09_local2")
    lax.fori_loop(4, 8, local_block, 0)
    phase("s10_waitrow")

    rdec_copies.wait()
    for earlier in range(1, 4):
        pl.when(z == earlier)(lambda: row_copies.wait(earlier * bytes_of(row_tx)))
    phase("s11_incoming")
    run = jnp.zeros((QUARTER, DV), F32)
    for at in range(4):
        later = jnp.exp(rdec_rx[at][0:1, 0:1]) * run + row_rx[at].astype(F32)
        run = jnp.where(at < z, later, run)
    for at in range(4):
        in_tx[at] = run.astype(BF16)
        if at < 3:
            run = jnp.exp(dec_rx[at][0:1, 0:1]) * run + st_rx[at].astype(F32)
    in_copies = net.group()
    for by in (2, 1, 3):
        to = step(y, by)
        net.start("state", in_copies, in_tx.at[to], in_rx.at[y], y=to)
    in_rx[y] = in_tx[y]

    phase("s13_waitin")
    f_wo.wait()
    f_gain.wait()
    in_copies.wait()
    phase("s12_w2wait")
    arrived(u1a)
    u1c = two("up", "y", twice(up_at(z, ym, 0)), twice(up_at(z, yp, 1)))
    f_dn.wait()
    d2_own = dn_out(z)
    arrived(u1b, d1b)
    u2_m, u2_p = up_out(ym), up_out(yp)
    d2_m, d2_p = dn_out(zm), dn_out(zp)
    def chunk(h):
        return slice(h * 64, h * 64 + 64)

    def project(d, h):
        picks = [pl.ds(pl.multiple_of(d * 256 + i * 128 + h * 64, 64), 64) for i in range(2)]

        def both(ref):
            return jnp.concatenate([ref[rows, :] for rows in picks], axis=0)

        incoming = jnp.concatenate([in_rx[at] for at in range(4)], axis=0)
        kept = both(local) + jnp.dot(both(q_late), incoming, preferred_element_type=F32)
        scale = lax.rsqrt(jnp.mean(kept * kept, axis=-1, keepdims=True) + EPS)
        gated[...] = (both(gate_f) * kept * scale).astype(BF16)
        for j in range(4):
            part = jnp.dot(
                gated[...], wo_s[:, j * 512 : (j + 1) * 512], preferred_element_type=F32
            ).astype(BF16)
            to = slice((j % 2) * 512, (j % 2) * 512 + 512)
            p1[h, d, 0, j // 2, :, to] = part[0:64]
            p1[h, d, 1, j // 2, :, to] = part[64:128]

    def mix_up(d, h):
        rows = normed[d, :, chunk(h), :].reshape(128, D)
        for j in range(2):
            cols = slice(j * 512, (j + 1) * 512)
            pre = jnp.maximum(jnp.dot(rows, up_w[:, cols], preferred_element_type=F32), 0.0)
            hidden[d, h, :, cols] = (pre * pre).astype(BF16)

    order = (y, ym, yp, step(y, 2))

    def dn_cols(k):
        return dn_w[:, pl.ds(pl.multiple_of(order[k] * 512, 512), 512)]

    def mix_down(d, h):
        for k in range(3):
            part = jnp.dot(hidden[d, h], dn_cols(k), preferred_element_type=F32).astype(BF16)
            for core in range(2):
                rows = slice(core * 64, core * 64 + 64)
                for at in range(0, 512, 256):
                    col = k * 512 + at
                    p2[h, d, core, col // 768, :, col % 768 : col % 768 + 256] = part[rows, at : at + 256]

    def mix_last(d, unused):
        part = jnp.dot(
            hidden[d].reshape(256, FFL), dn_cols(3), preferred_element_type=F32
        ).astype(BF16)
        for h in range(2):
            for core in range(2):
                at = h * 128 + core * 64
                for half in range(2):
                    p3[d, core, half, chunk(h), :] = part[at : at + 64, half * 256 : half * 256 + 256]

    class RingSum:
        blocks = {"xo": xo, "xp": xp, "xm": xm, "x": x}

        def __init__(self, name, compute, arg, p, p_rx, ra, rb):
            self.name, self.compute, self.arg = name, compute, arg
            self.p, self.p_rx = p, p_rx
            self.ra_p, self.ra_m, self.rb_p, self.rb_m = ra.at[0], ra.at[1], rb.at[0], rb.at[1]
            self.pairs, self.a, self.done = {}, net.group(), net.group()
            self.kind = name[0]

        def add(self, d, half, extra):
            total = self.p[d, c, half].astype(F32) + extra.astype(F32)
            self.p[d, c, half] = total.astype(BF16)

        def work(self, *keys):
            for key in keys:
                phase(f"{self.name}_work_{key}")
                d = self.blocks[key]
                self.compute(d, self.arg)
                self.pairs[key] = self.done if key == "x" else net.group()
                net.start(self.kind, self.pairs[key], self.p.at[d, other], self.p_rx.at[d], c=other)

        def pair_sum(self, key):
            phase(f"{self.name}_pair_{key}")
            d = self.blocks[key]
            self.pairs[key].wait()
            for half in range(2):
                self.add(d, half, self.p_rx[d, half])

        def piece(self, d, half):
            return self.p.at[d, c, half]

        def send(self, group, src, dst, to):
            net.start(self.kind, group, src, dst, x=to)

        def send_a(self):
            self.pair_sum("xo")
            self.send(self.a, self.piece(xo, 0), self.ra_p, xp)
            self.send(self.a, self.piece(xo, 1), self.ra_m, xm)

        def send_b(self):
            self.pair_sum("xp")
            self.send(self.done, self.piece(xp, 1), self.rb_p.at[1], xp)
            self.pair_sum("xm")
            self.send(self.done, self.piece(xm, 0), self.rb_m.at[0], xm)

        def send_c(self):
            phase(f"{self.name}_wait_a")
            self.a.wait()
            self.add(xp, 0, self.ra_p[...])
            self.send(self.done, self.piece(xp, 0), self.rb_p.at[0], xp)
            self.add(xm, 1, self.ra_m[...])
            self.send(self.done, self.piece(xm, 1), self.rb_m.at[1], xm)

        def complete(self):
            phase(f"{self.name}_wait_bc")
            self.done.wait()

        def total(self, half, rows, cols):
            value = self.p[x, c, half, rows, cols].astype(F32) + self.p_rx[x, half, rows, cols].astype(F32)
            sides = self.rb_p[half, rows, cols].astype(F32) + self.rb_m[half, rows, cols].astype(F32)
            return value + sides

    rings1 = [RingSum(f"p{h}", project, h, p1.at[h], p1_rx.at[h], ra1.at[h], rb1.at[h]) for h in range(2)]

    def norm_chunk(h):
        phase(f"n{h}_norm")
        gain = gain_s[...].astype(F32).reshape(1, D)
        for first in range(0, 64, 32):
            rows = slice(h * 64 + first, h * 64 + first + 32)
            halves = []
            for half in range(2):
                cols = slice(half * 1024, (half + 1) * 1024)
                value = rings1[h].total(half, slice(first, first + 32), slice(None))
                value = (resid_s[rows, cols].astype(F32) + value).astype(BF16)
                updated[rows, cols] = value
                halves.append(value.astype(F32))
            square = sum(jnp.sum(v * v, axis=-1, keepdims=True) for v in halves)
            scale = lax.rsqrt(square * (1.0 / D) + EPS)
            for half in range(2):
                cols = slice(half * 1024, (half + 1) * 1024)
                normed[x, c, rows, cols] = (halves[half] * scale * gain[:, cols]).astype(BF16)

    def rows_at(d, first, size):
        return twice(normed.at[d, c, first : first + size, :])

    def first_out(h):
        return two("gather", "x", rows_at(x, h * 64, 32), rows_at(x, h * 64 + 32, 32))

    def rest_out(h):
        return two("gather", "x", rows_at(x, h * 64 + 32, 32), rows_at(x, h * 64, 32))

    def pass_on(h):
        return two("gather", "x", rows_at(xm, h * 64, 32), rows_at(xp, h * 64 + 32, 32))

    def to_pair(d, h, group):
        net.start("gather", group, *rows_at(d, h * 64, 64), c=other)

    near = [net.group() for h in range(2)]
    far = [net.group() for h in range(2)]

    r0, r1 = rings1
    r0.work("xo", "xp")
    r0.send_a()
    r0.work("xm")
    r1.work("xo")
    r0.send_b()
    r1.work("xp")
    r1.send_a()
    r1.work("xm", "x")
    r0.work("x")
    phase("w_out_far")
    arrived(u1c, d1c)
    u2_o, d2_o = up_out(step(y, 2)), dn_out(step(z, 2))
    r0.send_c()
    r1.send_b()
    r1.send_c()
    phase("w_on_own")
    arrived(u2_own, d2_own)
    up_on(y)
    dn_on(z)
    r0.complete()
    norm_chunk(0)
    to_pair(x, 0, near[0])
    first0 = first_out(0)
    rest0 = rest_out(0)
    phase("w_on_minus")
    arrived(u2_m, d2_m)
    up_on(ym)
    dn_on(zm)
    r1.complete()
    norm_chunk(1)
    to_pair(x, 1, near[1])
    first1 = first_out(1)
    rest1 = rest_out(1)
    phase("w_on_plus")
    arrived(u2_p, d2_p)
    up_on(yp)
    dn_on(zp)
    phase("g0_wait_first")
    arrived(first0)
    on0 = pass_on(0)
    phase("w_on_far_u")
    arrived(u2_o)
    up_on(step(y, 2))
    phase("g0_wait_rest")
    arrived(rest0)
    for d in (xm, xp):
        to_pair(d, 0, near[0])
    phase("w_on_far_d")
    arrived(d2_o)
    dn_on(step(z, 2))
    phase("g1_wait_first")
    arrived(first1)
    on1 = pass_on(1)
    phase("g0_wait_pair")
    arrived(near[0])
    phase("w_wait_up")
    arrived(up_last)

    r0, r1 = [
        RingSum(f"m{h}", mix_down, h, p2.at[h], p2_rx.at[h], ra2.at[h], rb2.at[h]) for h in range(2)
    ]
    r2 = RingSum("m2", mix_last, None, p3, p3_rx, ra3, rb3)
    phase("m0_up_near")
    mix_up(xp, 0)
    mix_up(xm, 0)
    phase("g1_wait_rest")
    arrived(rest1)
    for d in (xm, xp):
        to_pair(d, 1, near[1])
    r0.work("xp", "xm")
    phase("g1_wait_pair")
    arrived(near[1])
    phase("m1_up_near")
    mix_up(xp, 1)
    mix_up(xm, 1)
    phase("g0_wait_on")
    arrived(on0)
    to_pair(xo, 0, far[0])
    r0.send_b()
    r1.work("xp", "xm")
    phase("g0_wait_far")
    arrived(far[0])
    phase("m0_up_far")
    mix_up(xo, 0)
    r0.work("xo")
    r1.send_b()
    phase("g1_wait_on")
    arrived(on1)
    to_pair(xo, 1, far[1])
    phase("m0_up_own")
    mix_up(x, 0)
    r0.send_a()
    phase("g1_wait_far")
    arrived(far[1])
    phase("m1_up_far")
    mix_up(xo, 1)
    r1.work("xo")
    phase("w_wait_last")
    arrived(dn_last)
    r2.work("xo", "xp")
    r1.send_a()
    r2.work("xm")
    r2.send_a()
    r0.send_c()
    phase("m1_up_own")
    mix_up(x, 1)
    r2.send_b()
    r1.send_c()
    r0.work("x")
    r1.work("x")
    r2.work("x")
    r2.send_c()

    def finish_columns(k, rows, total_at):
        for zz in range(4):
            cols = pl.ds(pl.multiple_of((4 * zz + order[k]) * 128, 128), 128)
            out_s[rows, cols] = (updated[rows, cols].astype(F32) + total_at(zz * 128)).astype(BF16)

    def chunk_total(ring, k):
        def at(first):
            col = k * 512 + first
            return ring.total(col // 768, slice(None), slice(col % 768, col % 768 + 128))

        return at

    for h, ring in enumerate((r0, r1)):
        ring.complete()
        phase(f"f{h}_final")
        for k in range(3):
            finish_columns(k, chunk(h), chunk_total(ring, k))
    r2.complete()
    phase("f2_final")
    finish_columns(3, slice(None), lambda first: r2.total(first // 256, slice(None), slice(first % 256, first % 256 + 128)))
    store = net.local_copies((out_s, out))
    phase("s35_finish")
    store.wait()
    net.finish()
    for count in range(1, 4):
        view = sized(count * bytes_of(row_tx))
        pl.when(z == 3 - count)(lambda: pltpu.make_async_copy(view, view, send.at[N_SEND - 1]).wait())
    phase(None)


def body(resid, q, k, v, g, log_decay, wo, gain, up, dn):
    vm = pltpu.VMEM
    scratch = [
        vm((ROWS, DK), BF16), vm((ROWS, DK), BF16), vm((ROWS, DV), BF16), vm((ROWS, DV), BF16),
        vm((DV, D), BF16), vm((128, D), BF16), vm((D,), BF16), vm((BLOCKS, 128), F32),
        vm((4, 128, 128), F32),
        vm((ROWS, 128), F32), vm((BLOCKS, 128), F32), vm((BLOCKS, 128), F32),
        vm((DK, DV), F32), vm((BLOCKS, DK, DV), BF16), vm((ROWS, DV), F32), vm((ROWS, DK), BF16),
        vm((128, DV), BF16), vm((ROWS, DV), F32),
        vm((4, QUARTER, DV), BF16), vm((4, QUARTER, DV), BF16),
        vm((4, QUARTER, DV), BF16), vm((4, QUARTER, DV), BF16),
        vm((QUARTER, DV), BF16), vm((4, QUARTER, DV), BF16),
        vm((8, 128), F32), vm((4, 8, 128), F32), vm((8, 128), F32), vm((4, 8, 128), F32),
        vm((2, 4, 2, 2, 64, 1024), BF16), vm((2, 4, 2, 64, 1024), BF16),
        vm((2, 2, 64, 1024), BF16), vm((2, 2, 2, 64, 1024), BF16),
        vm((128, D), BF16), vm((4, 2, 128, D), BF16), vm((4, 2, 128, FFL), BF16),
        vm((D, FFL), BF16), vm((FFL, D), BF16),
        vm((2, 4, 2, 2, 64, 768), BF16), vm((2, 4, 2, 64, 768), BF16),
        vm((2, 2, 64, 768), BF16), vm((2, 2, 2, 64, 768), BF16),
        vm((4, 2, 2, 128, 256), BF16), vm((4, 2, 128, 256), BF16),
        vm((2, 128, 256), BF16), vm((2, 2, 128, 256), BF16),
        vm((128, D), BF16),
        pltpu.SemaphoreType.DMA((N_SEND,)),
        pltpu.SemaphoreType.DMA((N_RECV,)),
        pltpu.SemaphoreType.DMA((N_LOCAL,)),
    ]
    anywhere = pl.BlockSpec(memory_space=pl.ANY)
    return pl.pallas_call(
        kernel,
        out_shape=jax.ShapeDtypeStruct((128, D), BF16),
        in_specs=[anywhere] * 11,
        out_specs=anywhere,
        scratch_shapes=scratch,
        compiler_params=pltpu.CompilerParams(
            collective_id=0, has_side_effects=True, vmem_limit_bytes=66_000_000
        ),
    )(
        resid, q, k, v, g, log_decay.reshape(BLOCKS, BLOCK), wo,
        gain, up, dn, jnp.asarray(rotation_tables()),
    )


def solution(mesh):
    torus = Mesh(mesh.devices.reshape(4, 4, 4, 2), ("z", "y", "x", "c"))
    sp, tp = ("z", "y"), ("x", "c")
    placed = (
        P(("z", "y", "x", "c"), None),
        P(sp, tp),
        P(sp, tp),
        P(sp, tp),
        P(sp, tp),
        P(tp, sp),
        P(tp, None),
        P(),
        P(sp, tp),
        P(tp, sp),
    )
    return jax.shard_map(
        body, mesh=torus, in_specs=placed, out_specs=P(("z", "y", "x", "c"), None), check_vma=False
    )
```
